512 devices in a mesh: ep: 32 (over z, core), tp: 16 (over y, x).
Axes of the slice: x: 4, y: 4, z: 16, core: 2. Of those that a mesh axis runs over, the one named last changes fastest.
Arguments:
- outer_gate: bfloat16 [4096, 2048], P('ep', 'tp'), may hold values from -6 to 6
- inner_gate: bfloat16 [4096, 2048], P('ep', 'tp'), may hold values from -6 to 6
- conv_value: bfloat16 [4096, 2048], P('ep', 'tp'), may hold values from -6 to 6
- conv_taps: bfloat16 [3, 2048], P(None, 'tp'), may hold values from -3.5 to 3.5
- mix_out: bfloat16 [2048, 2048], P(None, 'tp')
- gain_mixer: bfloat16 [2048], P('tp'), may hold values from 0.099609375 to 1.8984375
- bias_mixer: bfloat16 [2048], P('tp'), may hold values from -3 to 3
- moe_input: bfloat16 [4096, 2048], P('ep'), may hold values from -6 to 6
- route_ids: int32 [4096, 4], P('ep'), may hold values from 0 to 31, all different within a row; in each aligned block of 128 rows (0 to 127, 128 to 255, ...) at most 24 rows name the same one
- route_weights: float32 [4096, 4], P('ep'), may hold values from 0.1 to 1.2
- expert_gate: bfloat16 [32, 2048, 2048], P('ep', None, 'tp'), may hold values from -0.125 to 0.125
- expert_up: bfloat16 [32, 2048, 2048], P('ep', None, 'tp'), may hold values from -0.125 to 0.125
- expert_down: bfloat16 [32, 2048, 2048], P('ep', None, 'tp')
- shared_gate: bfloat16 [2048, 2048], P(None, 'tp'), may hold values from -0.125 to 0.125
- shared_up: bfloat16 [2048, 2048], P(None, 'tp'), may hold values from -0.125 to 0.125
- shared_down: bfloat16 [2048, 2048], P(None, 'tp')
- gain_experts: bfloat16 [2048], P('tp'), may hold values from 0.099609375 to 1.8984375
- bias_experts: bfloat16 [2048], P('tp'), may hold values from -3 to 3
Outputs:
- out_mixer: bfloat16 [4096, 2048], P('ep', 'tp')
- out_experts: bfloat16 [4096, 2048], P('ep', 'tp')
The draws below stay inside these ranges and needn't reach their ends.
Inputs may be any that keep to these rules, and one draw needn't show every extreme that they name: `route_ids`: each row names 4 different experts. Among the rows of one index of ep (aligned blocks of 128 rows) no expert is named more than 24 times, a bound that some block reaches.
All inputs are finite; a program needn't handle non-finite values.
Results may differ from the reference program's by a relative error of at most 0.0055.
Values may be sent and summed in bfloat16 or wider, within the bound.
No kernel may reach another device: no remote copies, remote signals or barrier semaphores. Data moves between devices by JAX's collectives and lax.ppermute only.
A program may use at most 64 MiB of HBM per device.

```python
import math
import jax
import jax.numpy as jnp
import numpy as np
from jax import lax

D = 2048
EFF = 2048
SFF = 2048
KERNEL = 3
TOPK = 4
ROWS = 128
TOKENS = 4096
EXPERTS = 32
CAP = 24
SEQ_LEN = 4096
N_EP = 32


def column_scales(key, width):
    place = jnp.arange(width, dtype=jnp.float32) / width
    rough = jax.random.uniform(jax.random.fold_in(key, 7), (width,), jnp.float32, 0.5, 2.0)
    return jnp.exp(jnp.log(10.0) * place) * rough


def draw_mix_out(key, part):
    values = jax.random.normal(jax.random.fold_in(key, 11), (D, D), jnp.float32) * D ** (-0.5)
    return (values * column_scales(key, D)[None, :]).astype(jnp.bfloat16)


def draw_expert_down(key, part):
    values = jax.random.normal(jax.random.fold_in(key, 13), (EXPERTS, EFF, D), jnp.float32) * EFF ** (-0.5)
    return (values * column_scales(key, D)[None, None, :]).astype(jnp.bfloat16)


def draw_shared_down(key, part):
    values = jax.random.normal(jax.random.fold_in(key, 17), (SFF, D), jnp.float32) * SFF ** (-0.5)
    return (values * column_scales(key, D)[None, :]).astype(jnp.bfloat16)


def level_of(rng, shape, shards, smallest, top_value):
    factor_of, own = 1.0, jax.random.fold_in(rng, 6)
    for position, parts in shards:
        steps = jnp.exp(jax.random.uniform(jax.random.fold_in(own, position), (parts,), jnp.float32, smallest / len(shards), top_value / len(shards)))
        factor_of = factor_of * jnp.repeat(steps, shape[position] // parts).reshape([-1 if axis == position else 1 for axis in range(len(shape))])
    return factor_of


def assign_block(own_key, own, number, rows, count, top, reach, skew):
    order = jax.random.permutation(own_key, count)
    heavy_load, common = shares(count, rows * top, reach, skew, True), shares(count, rows * top, reach, skew, False)
    places = jnp.arange(count)

    def named(lengths, turn):
        used = int((lengths > 0).sum())
        fixed = max(1, used // 4)
        passed = fixed + (places - fixed + turn * (used - fixed)) % max(1, count - fixed)
        return jnp.zeros((count,), jnp.int32).at[order[jnp.where(places < fixed, places, passed)]].set(jnp.asarray(lengths, jnp.int32))

    lengths = jnp.where(number % 4 == 0, named(heavy_load, number // 4), named(common, number - number // 4 - 1))
    mixed = jax.random.permutation(jax.random.fold_in(own, 3), count)
    donor, sink = mixed[0:count // 2 * 2:2], mixed[1:count // 2 * 2:2]
    room = jnp.minimum(lengths[donor] - 1, reach - lengths[sink]) // 2
    room = jnp.where((donor == order[0]) | (sink == order[0]) | (lengths[sink] == 0), 0, jnp.maximum(room, 0))
    passed = jax.random.randint(jax.random.fold_in(own, 4), (count // 2,), 0, 1 << 20) % (room + 1)
    lengths = lengths.at[donor].add(-passed).at[sink].add(passed)
    items = jnp.searchsorted(jnp.cumsum(lengths), jnp.arange(rows * top), side="right").astype(jnp.int32)
    grid = items.reshape(top, rows).T
    grid = grid[jax.random.permutation(jax.random.fold_in(own, 1), rows)]
    turn = jax.random.randint(jax.random.fold_in(own, 2), (rows, 1), 0, top)
    return jnp.take_along_axis(grid, (jnp.arange(top)[None, :] + turn) % top, axis=1)


def shares(number_of, total, reach, slope, full):
    portions = [(1 << 20) // math.isqrt(rank ** slope) + 1 for rank in range(1, number_of + 1)]
    largest = reach if full else min(reach, max(-(-total // number_of), total * portions[0] // sum(portions)))
    least = 1 if total - largest >= number_of - 1 else 0
    given, surplus = [largest] + [least] * (number_of - 1), total - largest - least * (number_of - 1)
    while surplus > 0:
        candidates = [i for i in range(1, number_of) if given[i] < largest] or [i for i in range(1, number_of) if given[i] < reach]
        mass, budget = sum([portions[i] for i in candidates]), surplus
        for i in candidates:
            addition = min(reach - given[i], max(1, budget * portions[i] // mass), surplus)
            given[i] = given[i] + addition
            surplus = surplus - addition
    return np.array(given)


def gaussian(own_key, shape, scale, bound, cuts=(), kind=jnp.bfloat16):
    drawn = jax.random.normal(own_key, shape, jnp.float32) * scale
    if len(cuts) > 0:
        drawn = level_of(own_key, shape, cuts, -0.22, 0.18) * drawn
    return jnp.clip(drawn, min=-bound, max=bound).astype(kind)


def setup_inputs(seed: int = 0) -> dict:
    key_list = jax.random.split(jax.random.key(seed), 19)
    outer_gate = gaussian(key_list[0], (TOKENS, D), 1.0, 6.0, ((0, 32), (1, 16)))
    inner_gate = gaussian(key_list[1], (TOKENS, D), 1.0, 6.0, ((0, 32), (1, 16)))
    conv_value = gaussian(key_list[2], (TOKENS, D), 1.0, 6.0, ((0, 32), (1, 16)))
    conv_taps = gaussian(key_list[3], (KERNEL, D), KERNEL ** -0.5, 3.5, ((1, 16),))
    mix_out = draw_mix_out(jax.random.fold_in(key_list[18], 71), 0)
    gain_mixer = jnp.clip(1.0 + 0.18 * jax.random.normal(key_list[5], (D,), jnp.float32), 0.099609375, 1.8984375).astype(jnp.bfloat16)
    bias_mixer = gaussian(key_list[6], (D,), 0.5, 3.0, ((0, 16),))
    moe_input = gaussian(key_list[7], (TOKENS, D), 1.0, 6.0, ((0, 32),))
    route_ids_keys = jax.random.split(jax.random.fold_in(key_list[8], 1), TOKENS // ROWS)
    route_ids_turns = jax.random.permutation(jax.random.fold_in(key_list[8], 3), TOKENS // ROWS)
    route_ids = jax.vmap(lambda own, number: assign_block(jax.random.fold_in(key_list[8], 2), own, number, ROWS, EXPERTS, TOPK, CAP, 1))(route_ids_keys, route_ids_turns).reshape((TOKENS, TOPK))
    route_weights = jnp.clip(0.1 + 1.1 * jax.random.uniform(key_list[9], (TOKENS, TOPK), jnp.float32) ** level_of(key_list[9], (TOKENS, TOPK), ((0, 32),), -0.2, 0.2), 0.1, 1.2)
    expert_gate = gaussian(key_list[10], (EXPERTS, D, EFF), D ** -0.5, 0.125, ((0, 32), (2, 16)))
    expert_up = gaussian(key_list[11], (EXPERTS, D, EFF), D ** -0.5, 0.125, ((0, 32), (2, 16)))
    expert_down = draw_expert_down(jax.random.fold_in(key_list[18], 71), 0)
    shared_gate = gaussian(key_list[13], (D, SFF), D ** -0.5, 0.125, ((1, 16),))
    shared_up = gaussian(key_list[14], (D, SFF), D ** -0.5, 0.125, ((1, 16),))
    shared_down = draw_shared_down(jax.random.fold_in(key_list[18], 71), 0)
    gain_experts = jnp.clip(1.0 + 0.18 * jax.random.normal(key_list[16], (D,), jnp.float32), 0.099609375, 1.8984375).astype(jnp.bfloat16)
    bias_experts = gaussian(key_list[17], (D,), 0.5, 3.0, ((0, 16),))
    return {"outer_gate": outer_gate, "inner_gate": inner_gate, "conv_value": conv_value, "conv_taps": conv_taps, "mix_out": mix_out, "gain_mixer": gain_mixer, "bias_mixer": bias_mixer, "moe_input": moe_input, "route_ids": route_ids, "route_weights": route_weights, "expert_gate": expert_gate, "expert_up": expert_up, "expert_down": expert_down, "shared_gate": shared_gate, "shared_up": shared_up, "shared_down": shared_down, "gain_experts": gain_experts, "bias_experts": bias_experts}


def row_norm(values, gain, offset_bias):
    average = lax.optimization_barrier(jnp.mean(values, axis=1, keepdims=True))
    spread = lax.optimization_barrier(jnp.mean(values * values, axis=1, keepdims=True)) - average * average
    scaled = (values - average) * lax.rsqrt(spread + 1e-05)
    return (scaled * gain.astype(jnp.float32) + offset_bias.astype(jnp.float32)).astype(jnp.bfloat16)

def rounded(value):
    narrow = lax.optimization_barrier(value.astype(jnp.bfloat16))
    return narrow.astype(jnp.float32)

def reference(outer_gate, inner_gate, conv_value, conv_taps, mix_out, gain_mixer, bias_mixer, moe_input, route_ids, route_weights, expert_gate, expert_up, expert_down, shared_gate, shared_up, shared_down, gain_experts, bias_experts):
    product = rounded(inner_gate.astype(jnp.float32) * conv_value.astype(jnp.float32))
    length = product.shape[0]
    places = jnp.arange(length, dtype=jnp.int32) % SEQ_LEN
    convolved = jnp.zeros(product.shape, jnp.float32)
    for offset in range(KERNEL):
        delay_rows = KERNEL - 1 - offset
        delayed = jnp.pad(product, ((delay_rows, 0), (0, 0)))[:length]
        kept_mask = (places >= delay_rows).astype(jnp.float32)[:, None]
        convolved = convolved + conv_taps[offset].astype(jnp.float32)[None, :] * delayed * kept_mask
    weighted_in = (outer_gate.astype(jnp.float32) * convolved).astype(jnp.bfloat16)
    mixed = jnp.dot(weighted_in, mix_out, preferred_element_type=jnp.float32)
    out_mixer = row_norm(mixed, gain_mixer, bias_mixer)
    flat_ids = route_ids.reshape(-1).astype(jnp.int32)
    count_all = flat_ids.shape[0]
    order = jnp.argsort(flat_ids, stable=True).astype(jnp.int32)
    marks = (flat_ids[:, None] == jnp.arange(EXPERTS, dtype=jnp.int32)[None, :]).astype(jnp.int32)
    counts = lax.optimization_barrier(jnp.sum(marks, axis=0)).astype(jnp.int32)
    starts = (jnp.cumsum(counts) - counts).astype(jnp.int32)
    most_rows = N_EP * CAP

    def one_expert(results, expert):
        slots = jnp.arange(most_rows, dtype=jnp.int32)
        picks = jnp.clip(starts[expert] + slots, 0, count_all - 1).astype(jnp.int32)
        assigned = order[picks]
        valid = slots < counts[expert]
        inputs = moe_input[assigned // TOPK]
        gate_value = jnp.dot(inputs, expert_gate[expert], preferred_element_type=jnp.float32)
        up_value = jnp.dot(inputs, expert_up[expert], preferred_element_type=jnp.float32)
        hidden = (jax.nn.silu(gate_value) * up_value).astype(jnp.bfloat16)
        output = jnp.dot(hidden, expert_down[expert], preferred_element_type=jnp.float32).astype(jnp.bfloat16)
        target = jnp.where(valid, assigned, count_all).astype(jnp.int32)
        return (results.at[target].set(output, mode='drop'), None)
    empty = jnp.zeros((count_all, D), jnp.bfloat16)
    routed = lax.scan(one_expert, empty, jnp.arange(EXPERTS, dtype=jnp.int32))[0]
    shared_gate_value = jnp.dot(moe_input, shared_gate, preferred_element_type=jnp.float32)
    shared_up_value = jnp.dot(moe_input, shared_up, preferred_element_type=jnp.float32)
    shared_hidden = (jax.nn.silu(shared_gate_value) * shared_up_value).astype(jnp.bfloat16)
    shared_sum = jnp.dot(shared_hidden, shared_down, preferred_element_type=jnp.float32)
    weighted = routed.reshape(-1, TOPK, D).astype(jnp.float32) * route_weights.astype(jnp.float32)[:, :, None]
    combined = lax.optimization_barrier(jnp.sum(weighted, axis=1)) + shared_sum
    out_experts = row_norm(combined, gain_experts, bias_experts)
    return (out_mixer, out_experts)
```

```python
import jax
import jax.numpy as jnp
from jax import lax
from jax.experimental import pallas as pl
from jax.experimental.pallas import tpu as pltpu
from jax.sharding import Mesh
from jax.sharding import PartitionSpec as P

SEQS = 1
F32 = jnp.float32
BF16 = jnp.bfloat16
TP = ("y", "x")


def shifted(block, axis, distance):
    devices = range(lax.axis_size(axis))
    route = [(i - distance, i) for i in devices if i - distance in devices]
    return lax.ppermute(block, axis, route)


def exchanged(x, axis):
    return lax.all_to_all(x, axis, split_axis=0, concat_axis=0, tiled=True)


def from_everyone(x, axis):
    return exchanged(jnp.broadcast_to(x, (lax.axis_size(axis), *x.shape)), axis)


def vmem(count):
    return [pl.BlockSpec(memory_space=pltpu.VMEM) for _ in range(count)]


def iota(shape, dim):
    return lax.broadcasted_iota(jnp.int32, shape, dim)


def ordinals(ids):
    rows = ids.shape[0]
    experts = iota((rows, 128), 1)
    named = jnp.zeros((rows, 128), F32)
    for k in range(ids.shape[1]):
        named = named + (ids[:, k : k + 1] == experts).astype(F32)
    before = (iota((rows, rows), 1) <= iota((rows, rows), 0)).astype(BF16)
    place = jnp.dot(before, named.astype(BF16), preferred_element_type=F32)
    return (named * place).astype(BF16), experts


def pack_kernel(where, ids_ref, x_ref, out_ref):
    slots, blocks = 6, 4
    rows = out_ref.shape[0]
    code, _ = ordinals(ids_ref[...])
    expert_of = (iota((rows, 128), 0) // (slots * blocks) == iota((rows, 128), 1)).astype(BF16)
    spread = lax.dot_general(
        expert_of, code, (((1,), (1,)), ((), ())), preferred_element_type=F32
    )
    row = iota(spread.shape, 0)
    wanted = (row % (slots * blocks)) // blocks + (where[0] * slots + 1)
    pick = (spread == wanted.astype(F32)).astype(BF16)
    taken = jnp.dot(pick, x_ref[...], preferred_element_type=F32)
    part = iota((rows, 128), 0) % blocks
    out = jnp.zeros((rows, 128), F32)
    for b in range(blocks):
        out = jnp.where(part == b, taken[:, b * 128 : (b + 1) * 128], out)
    out_ref[...] = out.astype(BF16)


def pack(where, ids, x):
    rows = ids.shape[0]
    return pl.pallas_call(
        pack_kernel,
        name="pack",
        out_shape=jax.ShapeDtypeStruct((768, 128), BF16),
        grid_spec=pltpu.PrefetchScalarGridSpec(
            num_scalar_prefetch=1,
            grid=(1,),
            in_specs=[
                pl.BlockSpec((rows, ids.shape[1]), lambda i, s: (0, 0)),
                pl.BlockSpec((rows, 512), lambda i, s: (0, s[1])),
            ],
            out_specs=pl.BlockSpec((768, 128), lambda i, s: (0, 0)),
        ),
    )(where, ids, x)


def hidden_kernel(x_ref, w_ref, out_ref, wide_ref, rows_ref):
    for q in range(4):
        wide_ref[...] = x_ref[q].astype(F32)
        for b in range(4):
            rows_ref[:, (q * 4 + b) * 128 : (q * 4 + b + 1) * 128] = wide_ref[
                pl.ds(b, 192, stride=4), :
            ].astype(BF16)
    rows = rows_ref[...]
    for y in range(4):
        gate = jnp.dot(rows, w_ref[y, 0], preferred_element_type=F32)
        up = jnp.dot(rows, w_ref[y, 1], preferred_element_type=F32)
        hidden = (gate / (1.0 + jnp.exp(-gate)) * up).astype(BF16)
        for q in range(4):
            out_ref[q, :, y * 128 : (y + 1) * 128] = hidden


def hidden_of(x, w):
    return pl.pallas_call(
        hidden_kernel,
        name="hidden",
        out_shape=jax.ShapeDtypeStruct((4, 192, 512), BF16),
        in_specs=vmem(2),
        out_specs=vmem(1)[0],
        scratch_shapes=[pltpu.VMEM((768, 128), F32), pltpu.VMEM((192, 2048), BF16)],
    )(x, w)


def down_kernel(h_ref, w_ref, out_ref, rows_ref, wide_ref):
    for q in range(4):
        for y in range(4):
            rows_ref[:, (y * 4 + q) * 128 : (y * 4 + q + 1) * 128] = h_ref[
                q, :, y * 128 : (y + 1) * 128
            ]
    rows = rows_ref[...]
    for y in range(4):
        wide_ref[pl.ds(y, 192, stride=4), :] = jnp.dot(
            rows, w_ref[y], preferred_element_type=F32
        )
    out_ref[...] = wide_ref[...].astype(BF16)


def down_of(h, w):
    return pl.pallas_call(
        down_kernel,
        name="down",
        out_shape=jax.ShapeDtypeStruct((768, 128), BF16),
        in_specs=vmem(2),
        out_specs=vmem(1)[0],
        scratch_shapes=[pltpu.VMEM((192, 2048), BF16), pltpu.VMEM((768, 128), F32)],
    )(h, w)


def combine_kernel(where, ids_ref, weights_ref, back_ref, out_ref):
    slots, blocks = 6, 4
    cols = back_ref.shape[0]
    ids = ids_ref[...]
    code, experts = ordinals(ids)
    weight = jnp.zeros(experts.shape, F32)
    for k in range(ids.shape[1]):
        weight = weight + jnp.where(
            ids[:, k : k + 1] == experts, weights_ref[:, k : k + 1], 0.0
        )
    expert_of = (iota((128, cols), 1) // (slots * blocks) == iota((128, cols), 0)).astype(BF16)
    spread = jnp.dot(code, expert_of, preferred_element_type=F32)
    col = iota(spread.shape, 1)
    wanted = (col % (slots * blocks)) // blocks + (where[0] * slots + 1)
    here = spread == wanted.astype(F32)
    parts = []
    for _ in range(3):
        piece = weight.astype(BF16)
        weight = weight - piece.astype(F32)
        spread_piece = jnp.dot(piece, expert_of, preferred_element_type=F32)
        parts.append(jnp.where(here, spread_piece, 0.0).astype(BF16))
    back = back_ref[...]
    for b in range(blocks):
        total = jnp.zeros((ids.shape[0], 128), F32)
        for piece in reversed(parts):
            mine = jnp.where(col % blocks == b, piece, jnp.zeros_like(piece))
            total = total + jnp.dot(mine, back, preferred_element_type=F32)
        out_ref[b] = total


def combine(where, ids, weights, back):
    rows = ids.shape[0]
    return pl.pallas_call(
        combine_kernel,
        name="combine",
        out_shape=jax.ShapeDtypeStruct((4, rows, 128), F32),
        in_specs=[pl.BlockSpec(memory_space=pltpu.SMEM)] + vmem(3),
        out_specs=vmem(1)[0],
    )(where, ids, weights, back)


def wide_kernel(parts_ref, mix_ref, shared_ref, mixed_ref, sum_ref, rows_ref):
    for half, (w_ref, out_ref) in enumerate(((mix_ref, mixed_ref), (shared_ref, sum_ref))):
        for p in range(16):
            rows_ref[:, p * 128 : (p + 1) * 128] = parts_ref[p, half * 128 : half * 128 + 128, :]
        out_ref[...] = jnp.dot(rows_ref[...], w_ref[...], preferred_element_type=F32)


def wide_products(parts, mix_out, shared_down):
    return pl.pallas_call(
        wide_kernel,
        name="wide",
        out_shape=[jax.ShapeDtypeStruct((128, 128), F32)] * 2,
        in_specs=vmem(3),
        out_specs=vmem(2),
        scratch_shapes=[pltpu.VMEM((128, 2048), BF16)],
    )(parts, mix_out, shared_down)


def stats_kernel(partial_ref, shared_ref, mixed_ref, combined_ref, out_ref):
    combined = shared_ref[...] + (
        (partial_ref[0] + partial_ref[1]) + (partial_ref[2] + partial_ref[3])
    )
    combined_ref[...] = combined
    for place, values in ((0, mixed_ref[...]), (2, combined)):
        turned = values.T
        total = jnp.sum(turned, axis=0, keepdims=True)
        square = jnp.sum(turned * turned, axis=0, keepdims=True)
        for p in range(16):
            out_ref[p, place : place + 1, :] = total
            out_ref[p, place + 1 : place + 2, :] = square


def stats_of(partial, shared, mixed):
    return pl.pallas_call(
        stats_kernel,
        name="stats",
        out_shape=[
            jax.ShapeDtypeStruct((128, 128), F32),
            jax.ShapeDtypeStruct((16, 4, 128), F32),
        ],
        in_specs=vmem(3),
        out_specs=vmem(2),
    )(partial, shared, mixed)


def finish_kernel(stats_ref, mixed_ref, combined_ref, coef_ref, out_mixer_ref, out_experts_ref):
    totals = stats_ref[0]
    for p in range(1, 16):
        totals = totals + stats_ref[p]
    totals = totals / 2048.0
    for place, values_ref, out_ref in (
        (0, mixed_ref, out_mixer_ref),
        (2, combined_ref, out_experts_ref),
    ):
        average = totals[place : place + 1]
        spread = totals[place + 1 : place + 2] - average * average
        scale = lax.rsqrt(spread + 1e-05)
        average = jnp.broadcast_to(average, (128, 128)).T
        scale = jnp.broadcast_to(scale, (128, 128)).T
        scaled = (values_ref[...] - average) * scale
        out_ref[...] = (
            scaled * coef_ref[place : place + 1, :] + coef_ref[place + 1 : place + 2, :]
        ).astype(BF16)


def finish(stats, mixed, combined, coef):
    return pl.pallas_call(
        finish_kernel,
        name="finish",
        out_shape=[jax.ShapeDtypeStruct((128, 128), BF16)] * 2,
        in_specs=vmem(4),
        out_specs=vmem(2),
    )(stats, mixed, combined, coef)


def on_device(
    outer_gate,
    inner_gate,
    conv_value,
    conv_taps,
    mix_out,
    gain_mixer,
    bias_mixer,
    moe_input,
    route_ids,
    route_weights,
    expert_gate,
    expert_up,
    expert_down,
    shared_gate,
    shared_up,
    shared_down,
    gain_experts,
    bias_experts,
):
    token_rows, column_count = outer_gate.shape
    ep_count = lax.axis_size("ep")
    taps_count = conv_taps.shape[0]
    where = jnp.stack([lax.axis_index("y"), lax.axis_index("x")]).astype(jnp.int32)

    sent = pack(where, route_ids, moe_input)
    arrived = exchanged(sent.reshape(ep_count, 24, 128), "ep").reshape(768, 128)
    into_hidden = from_everyone(jnp.concatenate([expert_gate, expert_up]), "y").reshape(4, 2, 2048, 128)
    into_out = from_everyone(expert_down[0], "y")

    product = (inner_gate.astype(F32) * conv_value.astype(F32)).astype(BF16)
    border = shifted(product[token_rows - (taps_count - 1) :], "ep", 1)
    extended = jnp.concatenate([border, product], axis=0).astype(F32)
    seq_length = token_rows * ep_count // SEQS
    places = (
        lax.axis_index("ep") * token_rows + jnp.arange(token_rows, dtype=jnp.int32)
    ) % seq_length
    convolved = jnp.zeros((token_rows, column_count), F32)
    for offset in range(taps_count):
        delay_rows = taps_count - 1 - offset
        delayed = extended[offset : offset + token_rows]
        kept_mask = (places >= delay_rows).astype(F32)[:, None]
        convolved = convolved + conv_taps[offset].astype(F32)[None, :] * delayed * kept_mask
    weighted_in = (outer_gate.astype(F32) * convolved).astype(BF16)
    shared_gate_value = jnp.dot(moe_input, shared_gate, preferred_element_type=F32)
    shared_up_value = jnp.dot(moe_input, shared_up, preferred_element_type=F32)
    shared_hidden = (jax.nn.silu(shared_gate_value) * shared_up_value).astype(BF16)
    both = from_everyone(jnp.concatenate([weighted_in, shared_hidden]), TP)
    mixed, shared_sum = wide_products(both, mix_out, shared_down)

    rows = from_everyone(arrived, "x")
    hidden = exchanged(hidden_of(rows, into_hidden), "x")
    expert_out = down_of(hidden, into_out)
    back = exchanged(expert_out.reshape(ep_count, 24, 128), "ep").reshape(768, 128)
    partial = exchanged(combine(where, route_ids, route_weights, back), "y")
    combined, stats = stats_of(partial, shared_sum, mixed)
    stats = exchanged(stats, TP)
    coef = jnp.stack([gain_mixer, bias_mixer, gain_experts, bias_experts]).astype(F32)
    return tuple(finish(stats, mixed, combined, coef))


def solution(mesh):
    split = Mesh(mesh.devices.reshape(mesh.shape["ep"], 4, 4), ("ep", "y", "x"))
    placed = (
        P("ep", TP),
        P("ep", TP),
        P("ep", TP),
        P(None, TP),
        P(None, TP),
        P(TP),
        P(TP),
        P("ep", None),
        P("ep", None),
        P("ep", None),
        P("ep", None, TP),
        P("ep", None, TP),
        P("ep", None, TP),
        P(None, TP),
        P(None, TP),
        P(None, TP),
        P(TP),
        P(TP),
    )
    return jax.shard_map(
        on_device,
        mesh=split,
        in_specs=placed,
        out_specs=(P("ep", TP), P("ep", TP)),
        check_vma=False,
    )
```

```python
import jax
import jax.numpy as jnp
from jax import lax
from jax.experimental import pallas as pl
from jax.experimental.pallas import tpu as pltpu
from jax.sharding import Mesh
from jax.sharding import PartitionSpec as P

SEQS = 1
F32 = jnp.float32
BF16 = jnp.bfloat16
TP = ("y", "x")
LIMIT = pltpu.CompilerParams(vmem_limit_bytes=20 * 2**20)


def shifted(block, axis, distance):
    devices = range(lax.axis_size(axis))
    route = [(i - distance, i) for i in devices if i - distance in devices]
    return lax.ppermute(block, axis, route)


def rotated(x, axis, distance):
    count = lax.axis_size(axis)
    return lax.ppermute(x, axis, [(i, (i + distance) % count) for i in range(count)])


def round_y(x):
    before, after = rotated(x, "y", 1), rotated(x, "y", -1)
    return before, after, rotated(before[0], "y", 1), rotated(after[1], "y", -1)


def exchanged(x, axis):
    return lax.all_to_all(x, axis, split_axis=0, concat_axis=0, tiled=True)


def vmem(count):
    return [pl.BlockSpec(memory_space=pltpu.VMEM) for _ in range(count)]


def near(*arrays):
    return [pltpu.with_memory_space_constraint(a, pltpu.VMEM) for a in arrays]


def iota(shape, dim):
    return lax.broadcasted_iota(jnp.int32, shape, dim)


def chunk(index, size):
    return pl.ds(pl.multiple_of(index * size, size), size)


SLOTS, BLOCKS = 6, 4


def ordinals(ids):
    tokens = ids.shape[1]
    experts = iota((32, tokens), 0)
    named = jnp.zeros((32, tokens), F32)
    for k in range(ids.shape[0]):
        named = named + (ids[k : k + 1, :] == experts).astype(F32)
    before = (iota((tokens, tokens), 0) <= iota((tokens, tokens), 1)).astype(BF16)
    place = jnp.dot(named.astype(BF16), before, preferred_element_type=F32)
    return (named * place).astype(BF16), experts


def slot_rows(code):
    rows = 32 * SLOTS * BLOCKS
    expert_of = (iota((rows, 32), 0) // (SLOTS * BLOCKS) == iota((rows, 32), 1)).astype(BF16)
    spread = jnp.dot(expert_of, code, preferred_element_type=F32)
    wanted = iota(spread.shape, 0) % (SLOTS * BLOCKS) // BLOCKS + (lax.axis_index("y") * SLOTS + 1)
    return expert_of, spread == wanted.astype(F32)


def pack_kernel(ids_ref, x_ref, out_ref):
    code, _ = ordinals(ids_ref[...])
    _, here = slot_rows(code)
    mine = x_ref[:, chunk(lax.axis_index("x"), 512)]
    taken = jnp.dot(here.astype(BF16), mine, preferred_element_type=F32)
    part = iota(out_ref.shape, 0) % BLOCKS
    out = taken[:, 0:128]
    for b in range(1, BLOCKS):
        out = jnp.where(part == b, taken[:, b * 128 : (b + 1) * 128], out)
    out_ref[...] = out.astype(BF16)


def pack(ids, x):
    return pl.pallas_call(
        pack_kernel,
        name="pack",
        compiler_params=LIMIT,
        out_shape=pltpu.VMEM((768, 128), BF16),
        in_specs=vmem(2),
        out_specs=vmem(1)[0],
    )(ids, x)


def copies_kernel(a_ref, b_ref, out_ref):
    for q in range(4):
        out_ref[q, 0:768, :] = a_ref[...]
        out_ref[q, 768:1024, :] = b_ref[...]


def copies(a, b):
    return pl.pallas_call(
        copies_kernel,
        name="copies",
        compiler_params=LIMIT,
        out_shape=pltpu.VMEM((4, 1024, 128), BF16),
        in_specs=vmem(2),
        out_specs=vmem(1)[0],
    )(*near(a, b))


def hidden_kernel(x_ref, gate_ref, up_ref, w1_ref, w2_ref, gate3_ref, up3_ref, out_ref, wide_ref, rows_ref):
    for q in range(4):
        wide_ref[...] = x_ref[q, 0:768, :].astype(F32)
        for b in range(4):
            rows_ref[:, (q * 4 + b) * 128 : (q * 4 + b + 1) * 128] = wide_ref[
                pl.ds(b, 192, stride=4), :
            ].astype(BF16)
    rows = rows_ref[...]
    pairs = (
        (gate_ref[0], up_ref[0]),
        (w1_ref[0], w1_ref[1]),
        (w2_ref[0], w2_ref[1]),
        (gate3_ref[...], up3_ref[...]),
    )
    for r, (gate_w, up_w) in enumerate(pairs):
        gate = jnp.dot(rows, gate_w, preferred_element_type=F32)
        up = jnp.dot(rows, up_w, preferred_element_type=F32)
        hidden = (gate / (1.0 + jnp.exp(-gate)) * up).astype(BF16)
        for q in range(4):
            out_ref[q, :, r * 128 : (r + 1) * 128] = hidden


def hidden_of(x, gate, up, w1, w2, gate3, up3):
    return pl.pallas_call(
        hidden_kernel,
        name="hidden",
        compiler_params=LIMIT,
        out_shape=pltpu.VMEM((4, 192, 512), BF16),
        in_specs=vmem(7),
        out_specs=vmem(1)[0],
        scratch_shapes=[pltpu.VMEM((768, 128), F32), pltpu.VMEM((192, 2048), BF16)],
    )(*near(x), gate, up, *near(w1, w2, gate3, up3))


def held_by(r):
    return (lax.axis_index("y") + (0, 3, 1, 2)[r]) % 4


def down_kernel(h_ref, w0_ref, w1_ref, w2_ref, low3_ref, high3_ref, out_ref, rows_ref, wide_ref, last_ref):
    for r in range(4):
        for q in range(4):
            rows_ref[:, (r * 4 + q) * 128 : (r * 4 + q + 1) * 128] = h_ref[
                q, :, r * 128 : (r + 1) * 128
            ]
    last_ref[0:1024, :] = low3_ref[...]
    last_ref[1024:2048, :] = high3_ref[...]
    for b, (w_ref) in enumerate((w0_ref.at[0], w1_ref, w2_ref, last_ref)):
        total = jnp.zeros((192, 128), F32)
        for r in range(4):
            total = total + jnp.dot(
                rows_ref[:, r * 512 : (r + 1) * 512],
                w_ref[chunk(held_by(r), 512), :],
                preferred_element_type=F32,
            )
        wide_ref[pl.ds(b, 192, stride=4), :] = total
    out_ref[...] = wide_ref[...].astype(BF16)


def down_of(h, w0, w1, w2, low3, high3):
    return pl.pallas_call(
        down_kernel,
        name="down",
        compiler_params=LIMIT,
        out_shape=pltpu.VMEM((768, 128), BF16),
        in_specs=vmem(6),
        out_specs=vmem(1)[0],
        scratch_shapes=[
            pltpu.VMEM((192, 2048), BF16),
            pltpu.VMEM((768, 128), F32),
            pltpu.VMEM((2048, 128), BF16),
        ],
    )(*near(h), w0, *near(w1, w2, low3, high3))


def combine_kernel(ids_ref, weights_ref, back_ref, out_ref):
    ids = ids_ref[...]
    code, experts = ordinals(ids)
    weight = jnp.zeros(experts.shape, F32)
    for k in range(ids.shape[0]):
        weight = weight + jnp.where(ids[k : k + 1, :] == experts, weights_ref[k : k + 1, :], 0.0)
    expert_of, here = slot_rows(code)
    block = iota(here.shape, 0) % BLOCKS
    parts = []
    for _ in range(3):
        piece = weight.astype(BF16)
        weight = weight - piece.astype(F32)
        parts.append(jnp.dot(expert_of, piece, preferred_element_type=F32))
    back = back_ref[...]
    for b in range(BLOCKS):
        total = jnp.zeros((128, 128), F32)
        for piece in reversed(parts):
            mine = jnp.where(here & (block == b), piece, 0.0).astype(BF16)
            total = total + lax.dot_general(
                mine, back, (((0,), (0,)), ((), ())), preferred_element_type=F32
            )
        out_ref[held_by(b)] = total


def combine(ids, weights, back):
    return pl.pallas_call(
        combine_kernel,
        name="combine",
        compiler_params=LIMIT,
        out_shape=pltpu.VMEM((4, 128, 128), F32),
        in_specs=vmem(3),
        out_specs=vmem(1)[0],
    )(ids, weights, *near(back))


def wide_kernel(own_ref, n1_ref, n2_ref, low3_ref, high3_ref, mix_ref, shared_ref, mixed_ref, sum_ref):
    for half, (w_ref, out_ref) in enumerate(((mix_ref, mixed_ref), (shared_ref, sum_ref))):
        total = jnp.zeros((128, 128), F32)
        last = (low3_ref, high3_ref)[half]
        for r, ref in enumerate((own_ref, n1_ref, n2_ref, last)):
            for q in range(4):
                if r == 0:
                    block = ref[q, 768 + half * 128 : 896 + half * 128, :]
                elif r < 3:
                    block = ref[half, q]
                else:
                    block = ref[q]
                total = total + jnp.dot(
                    block, w_ref[chunk(held_by(r) * 4 + q, 128), :], preferred_element_type=F32
                )
        out_ref[...] = total


def wide_products(own, n1, n2, low3, high3, mix_out, shared_down):
    return pl.pallas_call(
        wide_kernel,
        name="wide",
        compiler_params=LIMIT,
        out_shape=[pltpu.VMEM((128, 128), F32)] * 2,
        in_specs=vmem(7),
        out_specs=vmem(2),
    )(*near(own, n1, n2, low3, high3), mix_out, shared_down)


def stats_kernel(partial_ref, shared_ref, mixed_ref, combined_ref, out_ref):
    combined = shared_ref[...] + (
        (partial_ref[0] + partial_ref[1]) + (partial_ref[2] + partial_ref[3])
    )
    combined_ref[...] = combined
    for place, values in ((0, mixed_ref[...]), (2, combined)):
        turned = values.T
        total = jnp.sum(turned, axis=0, keepdims=True)
        square = jnp.sum(turned * turned, axis=0, keepdims=True)
        for p in range(16):
            out_ref[p, place : place + 1, :] = total
            out_ref[p, place + 1 : place + 2, :] = square


def stats_of(partial, shared, mixed):
    return pl.pallas_call(
        stats_kernel,
        name="stats",
        compiler_params=LIMIT,
        out_shape=[pltpu.VMEM((128, 128), F32), pltpu.VMEM((16, 4, 128), F32)],
        in_specs=vmem(3),
        out_specs=vmem(2),
    )(*near(partial, shared, mixed))


def finish_kernel(stats_ref, mixed_ref, combined_ref, coef_ref, out_mixer_ref, out_experts_ref):
    totals = stats_ref[0]
    for p in range(1, 16):
        totals = totals + stats_ref[p]
    totals = totals / 2048.0
    for place, values_ref, out_ref in (
        (0, mixed_ref, out_mixer_ref),
        (2, combined_ref, out_experts_ref),
    ):
        average = totals[place : place + 1]
        spread = totals[place + 1 : place + 2] - average * average
        scale = lax.rsqrt(spread + 1e-05)
        average = jnp.broadcast_to(average, (128, 128)).T
        scale = jnp.broadcast_to(scale, (128, 128)).T
        scaled = (values_ref[...] - average) * scale
        out_ref[...] = (
            scaled * coef_ref[place : place + 1, :] + coef_ref[place + 1 : place + 2, :]
        ).astype(BF16)


def finish(stats, mixed, combined, coef):
    return pl.pallas_call(
        finish_kernel,
        name="finish",
        compiler_params=LIMIT,
        out_shape=[jax.ShapeDtypeStruct((128, 128), BF16)] * 2,
        in_specs=vmem(4),
        out_specs=vmem(2),
    )(*near(stats, mixed, combined), coef)


def on_device(
    outer_gate,
    inner_gate,
    conv_value,
    conv_taps,
    mix_out,
    gain_mixer,
    bias_mixer,
    moe_input,
    route_ids,
    route_weights,
    expert_gate,
    expert_up,
    expert_down,
    shared_gate,
    shared_up,
    shared_down,
    gain_experts,
    bias_experts,
):
    token_rows, column_count = outer_gate.shape
    ep_count = lax.axis_size("ep")
    taps_count = conv_taps.shape[0]
    ids = route_ids.T
    sent = pack(ids, moe_input)
    sent, gate_now, up_now = lax.optimization_barrier((sent, expert_gate, expert_up))
    into_hidden = jnp.concatenate([gate_now, up_now])
    arrived = exchanged(sent.reshape(ep_count, 24, 128), "ep").reshape(768, 128)
    w1, w2, gate3, up3 = round_y(into_hidden)
    v1, v2, low3, high3 = round_y(expert_down.reshape(2, 1024, 128))

    product = (inner_gate.astype(F32) * conv_value.astype(F32)).astype(BF16)
    border = shifted(product[token_rows - (taps_count - 1) :], "ep", 1)
    extended = jnp.concatenate([border, product], axis=0).astype(F32)
    seq_length = token_rows * ep_count // SEQS
    places = (
        lax.axis_index("ep") * token_rows + jnp.arange(token_rows, dtype=jnp.int32)
    ) % seq_length
    convolved = jnp.zeros((token_rows, column_count), F32)
    for offset in range(taps_count):
        delay_rows = taps_count - 1 - offset
        delayed = extended[offset : offset + token_rows]
        kept_mask = (places >= delay_rows).astype(F32)[:, None]
        convolved = convolved + conv_taps[offset].astype(F32)[None, :] * delayed * kept_mask
    weighted_in = (outer_gate.astype(F32) * convolved).astype(BF16)
    shared_gate_value = jnp.dot(moe_input, shared_gate, preferred_element_type=F32)
    shared_up_value = jnp.dot(moe_input, shared_up, preferred_element_type=F32)
    shared_hidden = (jax.nn.silu(shared_gate_value) * shared_up_value).astype(BF16)
    both = jnp.concatenate([weighted_in, shared_hidden])
    rows = exchanged(copies(arrived, both), "x")
    wide = jnp.moveaxis(rows[:, 768:].reshape(4, 2, 128, 128), 1, 0)
    n1, n2, mix3, shared3 = round_y(wide)
    mixed, shared_sum = wide_products(rows, n1, n2, mix3, shared3, mix_out, shared_down)

    hidden = exchanged(hidden_of(rows, expert_gate, expert_up, w1, w2, gate3, up3), "x")
    expert_out = down_of(
        hidden, expert_down, v1.reshape(2048, 128), v2.reshape(2048, 128), low3, high3
    )
    back = exchanged(expert_out.reshape(ep_count, 24, 128), "ep").reshape(768, 128)
    partial = exchanged(combine(ids, route_weights.T, back), "y")
    combined, stats = stats_of(partial, shared_sum, mixed)
    stats = exchanged(stats, TP)
    coef = jnp.stack([gain_mixer, bias_mixer, gain_experts, bias_experts]).astype(F32)
    return tuple(finish(stats, mixed, combined, coef))


def solution(mesh):
    split = Mesh(mesh.devices.reshape(mesh.shape["ep"], 4, 4), ("ep", "y", "x"))
    placed = (
        P("ep", TP),
        P("ep", TP),
        P("ep", TP),
        P(None, TP),
        P(None, TP),
        P(TP),
        P(TP),
        P("ep", None),
        P("ep", None),
        P("ep", None),
        P("ep", None, TP),
        P("ep", None, TP),
        P("ep", None, TP),
        P(None, TP),
        P(None, TP),
        P(None, TP),
        P(TP),
        P(TP),
    )
    return jax.shard_map(
        on_device,
        mesh=split,
        in_specs=placed,
        out_specs=(P("ep", TP), P("ep", TP)),
        check_vma=False,
    )
```

```python
import jax
import jax.numpy as jnp
from jax import lax
from jax.experimental import pallas as pl
from jax.experimental.pallas import tpu as pltpu
from jax.sharding import Mesh
from jax.sharding import PartitionSpec as P


SEQS = 1
F32 = jnp.float32
BF16 = jnp.bfloat16
TP = ("y", "x")
LIMIT = pltpu.CompilerParams(vmem_limit_bytes=20 * 2**20)


def shifted(block, axis, distance):
    devices = range(lax.axis_size(axis))
    route = [(i - distance, i) for i in devices if i - distance in devices]
    return lax.ppermute(block, axis, route)


def rotated(x, distance):
    count = lax.axis_size("y")
    return lax.ppermute(x, "y", [(i, (i + distance) % count) for i in range(count)])


def exchanged(x, axis):
    return lax.all_to_all(x, axis, split_axis=0, concat_axis=0, tiled=True)


def vmem(count):
    return [pl.BlockSpec(memory_space=pltpu.VMEM) for _ in range(count)]


def near(*arrays):
    return [pltpu.with_memory_space_constraint(a, pltpu.VMEM) for a in arrays]


def iota(shape, dim):
    return lax.broadcasted_iota(jnp.int32, shape, dim)


def chunk(index, size):
    return pl.ds(pl.multiple_of(index * size, size), size)


SLOTS, BLOCKS = 6, 4


def ordinals(ids):
    tokens = ids.shape[1]
    experts = iota((32, tokens), 0)
    named = jnp.zeros((32, tokens), F32)
    for k in range(ids.shape[0]):
        named = named + (ids[k : k + 1, :] == experts).astype(F32)
    before = (iota((tokens, tokens), 0) <= iota((tokens, tokens), 1)).astype(BF16)
    place = jnp.dot(named.astype(BF16), before, preferred_element_type=F32)
    return (named * place).astype(BF16), experts


def spread_over(code, rows, each):
    expert_of = (iota((rows, 32), 0) // each == iota((rows, 32), 1)).astype(BF16)
    return expert_of, jnp.dot(expert_of, code, preferred_element_type=F32)


def pack_kernel(ids_ref, x_hbm, gate_hbm, up_hbm, out_ref, stack_ref, x_ref, sems):
    moves = (
        pltpu.make_async_copy(x_hbm.at[:, chunk(lax.axis_index("x"), 512)], x_ref, sems.at[0]),
        pltpu.make_async_copy(gate_hbm.at[0], stack_ref.at[0], sems.at[1]),
        pltpu.make_async_copy(gate_hbm.at[1], stack_ref.at[1], sems.at[2]),
        pltpu.make_async_copy(up_hbm.at[0], stack_ref.at[2], sems.at[3]),
        pltpu.make_async_copy(up_hbm.at[1], stack_ref.at[3], sems.at[4]),
    )
    for move in moves:
        move.start()
    code, _ = ordinals(ids_ref[...])
    _, spread = spread_over(code, 32 * SLOTS * BLOCKS, SLOTS * BLOCKS)
    wanted = iota(spread.shape, 0) % (SLOTS * BLOCKS) // BLOCKS + (lax.axis_index("y") * SLOTS + 1)
    here = (spread == wanted.astype(F32)).astype(BF16)
    moves[0].wait()
    taken = jnp.dot(here, x_ref[...], preferred_element_type=F32)
    part = iota(out_ref.shape, 0) % BLOCKS
    out = taken[:, 0:128]
    for b in range(1, BLOCKS):
        out = jnp.where(part == b, taken[:, b * 128 : (b + 1) * 128], out)
    out_ref[...] = out.astype(BF16)
    for move in moves[1:]:
        move.wait()


def pack(ids, x, gate, up):
    anywhere = pl.BlockSpec(memory_space=pltpu.HBM)
    return pl.pallas_call(
        pack_kernel,
        name="pack",
        compiler_params=LIMIT,
        out_shape=[pltpu.VMEM((768, 128), BF16), pltpu.VMEM((4, 1024, 128), BF16)],
        in_specs=vmem(1) + [anywhere] * 3,
        out_specs=vmem(2),
        scratch_shapes=[pltpu.VMEM((128, 512), BF16), pltpu.SemaphoreType.DMA((5,))],
    )(ids, *(pltpu.with_memory_space_constraint(a, pltpu.HBM) for a in (x, gate, up)))


def copies_kernel(a_ref, b_ref, out_ref):
    for q in range(4):
        out_ref[q, 0:768, :] = a_ref[...]
        out_ref[q, 768:1024, :] = b_ref[...]


def copies(a, b):
    return pl.pallas_call(
        copies_kernel,
        name="copies",
        compiler_params=LIMIT,
        out_shape=pltpu.VMEM((4, 1024, 128), BF16),
        in_specs=vmem(2),
        out_specs=vmem(1)[0],
    )(*near(a, b))


def hidden_kernel(x_ref, gate_ref, up_ref, w1_ref, w2_ref, gate3_ref, up3_ref, out_ref, wide_ref, rows_ref):
    for q in range(4):
        wide_ref[...] = x_ref[q, 0:768, :].astype(F32)
        for b in range(4):
            rows_ref[:, (q * 4 + b) * 128 : (q * 4 + b + 1) * 128] = wide_ref[
                pl.ds(b, 192, stride=4), :
            ].astype(BF16)
    rows = rows_ref[...]
    pairs = (
        (gate_ref[0], up_ref[0]),
        (w1_ref[0:2].reshape(2048, 128), w1_ref[2:4].reshape(2048, 128)),
        (w2_ref[0:2].reshape(2048, 128), w2_ref[2:4].reshape(2048, 128)),
        (gate3_ref[...].reshape(2048, 128), up3_ref[...].reshape(2048, 128)),
    )
    for r, (gate_w, up_w) in enumerate(pairs):
        gate = jnp.dot(rows, gate_w, preferred_element_type=F32)
        up = jnp.dot(rows, up_w, preferred_element_type=F32)
        hidden = (gate / (1.0 + jnp.exp(-gate)) * up).astype(BF16)
        for q in range(4):
            out_ref[q, :, r * 128 : (r + 1) * 128] = hidden


def hidden_of(x, *weights):
    return pl.pallas_call(
        hidden_kernel,
        name="hidden",
        compiler_params=LIMIT,
        out_shape=pltpu.VMEM((4, 192, 512), BF16),
        in_specs=vmem(7),
        out_specs=vmem(1)[0],
        scratch_shapes=[pltpu.VMEM((768, 128), F32), pltpu.VMEM((192, 2048), BF16)],
    )(*near(x), *weights)


def held_by(r):
    return (lax.axis_index("y") + (0, 3, 1, 2)[r]) % 4


def down_kernel(h_ref, w0_ref, w1_ref, w2_ref, w3_ref, out_ref, rows_ref):
    for r in range(4):
        for q in range(4):
            rows_ref[:, (r * 4 + q) * 128 : (r * 4 + q + 1) * 128] = h_ref[
                q, :, r * 128 : (r + 1) * 128
            ]
    to, of = iota((256, 192), 0), iota((256, 192), 1)
    place = ((to // 8 == of // SLOTS) & (to % 8 == of % SLOTS)).astype(BF16)
    for b, w_ref in enumerate((w0_ref, w1_ref, w2_ref, w3_ref)):
        total = jnp.zeros((192, 128), F32)
        for r in range(4):
            total = total + jnp.dot(
                rows_ref[:, r * 512 : (r + 1) * 512],
                w_ref[0, chunk(held_by(r), 512), :],
                preferred_element_type=F32,
            )
        placed = jnp.dot(place, total.astype(BF16), preferred_element_type=F32)
        out_ref[:, held_by(b)] = placed.astype(BF16).reshape(32, 8, 128)


def down_of(h, *weights):
    return pl.pallas_call(
        down_kernel,
        name="down",
        compiler_params=LIMIT,
        out_shape=pltpu.VMEM((32, 4, 8, 128), BF16),
        in_specs=vmem(5),
        out_specs=vmem(1)[0],
        scratch_shapes=[pltpu.VMEM((192, 2048), BF16)],
    )(*near(h), *weights)


def wide_kernel(own_ref, n1_ref, n2_ref, n3_ref, mix_ref, shared_ref, mixed_ref, sum_ref):
    for half, (w_ref, out_ref) in enumerate(((mix_ref, mixed_ref), (shared_ref, sum_ref))):
        total = jnp.zeros((128, 128), F32)
        for r, ref in enumerate((own_ref, n1_ref, n2_ref, n3_ref)):
            start = half * 128
            for q in range(4):
                total = total + jnp.dot(
                    ref[q, start : start + 128, :],
                    w_ref[chunk(held_by(r) * 4 + q, 128), :],
                    preferred_element_type=F32,
                )
        out_ref[...] = total


def wide_products(own, n1, n2, n3, mix_out, shared_down):
    return pl.pallas_call(
        wide_kernel,
        name="wide",
        compiler_params=LIMIT,
        out_shape=[pltpu.VMEM((128, 128), F32)] * 2,
        in_specs=vmem(6),
        out_specs=vmem(2),
    )(*near(own, n1, n2, n3), mix_out, shared_down)


def combine_kernel(ids_ref, weights_ref, back_ref, shared_ref, mixed_ref, combined_ref, out_ref):
    ids = ids_ref[...]
    code, experts = ordinals(ids)
    weight = jnp.zeros(experts.shape, F32)
    for k in range(ids.shape[0]):
        weight = weight + jnp.where(ids[k : k + 1, :] == experts, weights_ref[k : k + 1, :], 0.0)
    expert_of, spread = spread_over(code, 1024, 32)
    row = iota(spread.shape, 0)
    wanted = row % 32 // 8 * SLOTS + row % 8 + 1
    here = (spread == wanted.astype(F32)) & (row % 8 < SLOTS)
    back = back_ref[...].reshape(1024, 128)
    pieces = []
    for _ in range(3):
        piece = weight.astype(BF16)
        weight = weight - piece.astype(F32)
        piece = jnp.dot(expert_of, piece, preferred_element_type=F32)
        pieces.append(jnp.where(here, piece, 0.0).astype(BF16))
    routed = jnp.zeros((128, 128), F32)
    for piece in reversed(pieces):
        routed = routed + lax.dot_general(
            piece, back, (((0,), (0,)), ((), ())), preferred_element_type=F32
        )
    combined = routed + shared_ref[...]
    combined_ref[...] = combined
    for place, values in ((0, mixed_ref[...]), (2, combined)):
        turned = values.T
        total = jnp.sum(turned, axis=0, keepdims=True)
        square = jnp.sum(turned * turned, axis=0, keepdims=True)
        for p in range(16):
            out_ref[p, place : place + 1, :] = total
            out_ref[p, place + 1 : place + 2, :] = square


def combine(ids, weights, back, shared, mixed):
    return pl.pallas_call(
        combine_kernel,
        name="combine",
        compiler_params=LIMIT,
        out_shape=[pltpu.VMEM((128, 128), F32), pltpu.VMEM((16, 4, 128), F32)],
        in_specs=vmem(5),
        out_specs=vmem(2),
    )(ids, weights, *near(back, shared, mixed))


def finish_kernel(stats_ref, mixed_ref, combined_ref, coef_ref, out_mixer_ref, out_experts_ref):
    totals = stats_ref[0]
    for p in range(1, 16):
        totals = totals + stats_ref[p]
    totals = totals / 2048.0
    for place, values_ref, out_ref in (
        (0, mixed_ref, out_mixer_ref),
        (2, combined_ref, out_experts_ref),
    ):
        average = totals[place : place + 1]
        spread = totals[place + 1 : place + 2] - average * average
        scale = lax.rsqrt(spread + 1e-05)
        average = jnp.broadcast_to(average, (128, 128)).T
        scale = jnp.broadcast_to(scale, (128, 128)).T
        scaled = (values_ref[...] - average) * scale
        out_ref[...] = (
            scaled * coef_ref[place : place + 1, :] + coef_ref[place + 1 : place + 2, :]
        ).astype(BF16)


def finish(stats, mixed, combined, coef):
    return pl.pallas_call(
        finish_kernel,
        name="finish",
        compiler_params=LIMIT,
        out_shape=[jax.ShapeDtypeStruct((128, 128), BF16)] * 2,
        in_specs=vmem(4),
        out_specs=vmem(2),
    )(*near(stats, mixed, combined), coef)


def on_device(
    outer_gate,
    inner_gate,
    conv_value,
    conv_taps,
    mix_out,
    gain_mixer,
    bias_mixer,
    moe_input,
    route_ids,
    route_weights,
    expert_gate,
    expert_up,
    expert_down,
    shared_gate,
    shared_up,
    shared_down,
    gain_experts,
    bias_experts,
):
    token_rows, column_count = outer_gate.shape
    ep_count = lax.axis_size("ep")
    taps_count = conv_taps.shape[0]
    ids = route_ids.T
    sent, own = pack(
        ids, moe_input, expert_gate.reshape(2, 1024, 128), expert_up.reshape(2, 1024, 128)
    )
    arrived = exchanged(sent.reshape(ep_count, 24, 128), "ep").reshape(768, 128)
    before, after = rotated(own, 1), rotated(own, -1)
    far_gate = before[0:2]
    far_up = after[2:4]
    gate3, up3 = rotated(far_gate, 1), rotated(far_up, -1)
    down1, down2 = rotated(expert_down, 1), rotated(expert_down, -1)
    down3 = rotated(expert_down, 2)

    product = (inner_gate.astype(F32) * conv_value.astype(F32)).astype(BF16)
    border = shifted(product[token_rows - (taps_count - 1) :], "ep", 1)
    extended = jnp.concatenate([border, product], axis=0).astype(F32)
    seq_length = token_rows * ep_count // SEQS
    places = (
        lax.axis_index("ep") * token_rows + jnp.arange(token_rows, dtype=jnp.int32)
    ) % seq_length
    convolved = jnp.zeros((token_rows, column_count), F32)
    for offset in range(taps_count):
        delay_rows = taps_count - 1 - offset
        delayed = extended[offset : offset + token_rows]
        kept_mask = (places >= delay_rows).astype(F32)[:, None]
        convolved = convolved + conv_taps[offset].astype(F32)[None, :] * delayed * kept_mask
    weighted_in = (outer_gate.astype(F32) * convolved).astype(BF16)
    shared_gate_value = jnp.dot(moe_input, shared_gate, preferred_element_type=F32)
    shared_up_value = jnp.dot(moe_input, shared_up, preferred_element_type=F32)
    shared_hidden = (jax.nn.silu(shared_gate_value) * shared_up_value).astype(BF16)
    both = jnp.concatenate([weighted_in, shared_hidden])
    rows = exchanged(copies(arrived, both), "x")
    wide = rows[:, 768:]
    mixed, shared_sum = wide_products(
        wide, rotated(wide, 1), rotated(wide, -1), rotated(wide, 2), mix_out, shared_down
    )
    hidden = hidden_of(rows, expert_gate, expert_up, before, after, gate3, up3)
    hidden = exchanged(hidden, "x")
    expert_out = down_of(hidden, expert_down, down1, down2, down3)
    back = exchanged(expert_out.reshape(ep_count * 4, 8, 128), ("ep", "y"))
    combined, stats = combine(ids, route_weights.T, back, shared_sum, mixed)
    stats = exchanged(stats, TP)
    coef = jnp.stack([gain_mixer, bias_mixer, gain_experts, bias_experts]).astype(F32)
    return tuple(finish(stats, mixed, combined, coef))


def solution(mesh):
    split = Mesh(mesh.devices.reshape(mesh.shape["ep"], 4, 4), ("ep", "y", "x"))
    placed = (
        P("ep", TP),
        P("ep", TP),
        P("ep", TP),
        P(None, TP),
        P(None, TP),
        P(TP),
        P(TP),
        P("ep", None),
        P("ep", None),
        P("ep", None),
        P("ep", None, TP),
        P("ep", None, TP),
        P("ep", None, TP),
        P(None, TP),
        P(None, TP),
        P(None, TP),
        P(TP),
        P(TP),
    )
    return jax.shard_map(
        on_device,
        mesh=split,
        in_specs=placed,
        out_specs=(P("ep", TP), P("ep", TP)),
        check_vma=False,
    )
```

```python
import jax
import jax.numpy as jnp
from jax import lax
from jax.experimental import pallas as pl
from jax.experimental.pallas import tpu as pltpu
from jax.sharding import Mesh
from jax.sharding import PartitionSpec as P


F32 = jnp.float32
BF16 = jnp.bfloat16
TP = ("y", "x")
LIMIT = pltpu.CompilerParams(vmem_limit_bytes=20 * 2**20)


def shifted(block, axis, distance):
    devices = range(lax.axis_size(axis))
    route = [(i - distance, i) for i in devices if i - distance in devices]
    return lax.ppermute(block, axis, route)


def rotated(x, distance):
    count = lax.axis_size("y")
    return lax.ppermute(x, "y", [(i, (i + distance) % count) for i in range(count)])


def exchanged(x, axis):
    return lax.all_to_all(x, axis, split_axis=0, concat_axis=0, tiled=True)


def vmem(count):
    return [pl.BlockSpec(memory_space=pltpu.VMEM) for _ in range(count)]


def near(*arrays):
    return [pltpu.with_memory_space_constraint(a, pltpu.VMEM) for a in arrays]


def iota(shape, dim):
    return lax.broadcasted_iota(jnp.int32, shape, dim)


def chunk(index, size):
    return pl.ds(pl.multiple_of(index * size, size), size)


SLOTS, BLOCKS = 6, 4


def ordinals(ids):
    tokens = ids.shape[1]
    experts = iota((32, tokens), 0)
    named = jnp.zeros((32, tokens), F32)
    for k in range(ids.shape[0]):
        named = named + (ids[k : k + 1, :] == experts).astype(F32)
    before = (iota((tokens, tokens), 0) <= iota((tokens, tokens), 1)).astype(BF16)
    place = jnp.dot(named.astype(BF16), before, preferred_element_type=F32)
    return (named * place).astype(BF16), experts


def spread_over(code, rows, each):
    expert_of = (iota((rows, 32), 0) // each == iota((rows, 32), 1)).astype(BF16)
    return expert_of, jnp.dot(expert_of, code, preferred_element_type=F32)


def side_by_side(gate_hbm, up_hbm, stack_ref, sems):
    return tuple(
        pltpu.make_async_copy(
            ref.at[half * 1024 : half * 1024 + 1024],
            stack_ref.at[half * 1024 : half * 1024 + 1024, side * 128 : side * 128 + 128],
            sems.at[2 * side + half],
        )
        for side, ref in enumerate((gate_hbm, up_hbm))
        for half in range(2)
    )


def far(*arrays):
    return [pltpu.with_memory_space_constraint(a, pltpu.HBM) for a in arrays]


def hbm(count):
    return [pl.BlockSpec(memory_space=pltpu.HBM) for _ in range(count)]


def pack_kernel(
    ids_hbm, x_hbm, gate_hbm, up_hbm, out_ref, stack_ref, ids_ref, x_ref, first_sem, sem, sems
):
    first = pltpu.make_async_copy(ids_hbm, ids_ref, first_sem)
    first.start()
    mine = pltpu.make_async_copy(x_hbm.at[:, chunk(lax.axis_index("x"), 512)], x_ref, sem)
    mine.start()
    moves = side_by_side(gate_hbm, up_hbm, stack_ref, sems)
    for move in moves:
        move.start()
    first.wait()
    code, _ = ordinals(ids_ref[...])
    _, spread = spread_over(code, 32 * SLOTS * BLOCKS, SLOTS * BLOCKS)
    wanted = iota(spread.shape, 0) % (SLOTS * BLOCKS) // BLOCKS + (lax.axis_index("y") * SLOTS + 1)
    here = (spread == wanted.astype(F32)).astype(BF16)
    mine.wait()
    taken = jnp.dot(here, x_ref[...], preferred_element_type=F32)
    part = iota(out_ref.shape, 0) % BLOCKS
    out = taken[:, 0:128]
    for b in range(1, BLOCKS):
        out = jnp.where(part == b, taken[:, b * 128 : (b + 1) * 128], out)
    out_ref[...] = out.astype(BF16)
    for move in moves:
        move.wait()


def pack(ids, x, gate, up):
    return pl.pallas_call(
        pack_kernel,
        name="pack",
        compiler_params=LIMIT,
        out_shape=[pltpu.HBM((768, 128), BF16), pltpu.VMEM((2048, 256), BF16)],
        in_specs=hbm(4),
        out_specs=vmem(2),
        scratch_shapes=[
            pltpu.VMEM((4, 128), jnp.int32),
            pltpu.VMEM((128, 512), BF16),
            pltpu.SemaphoreType.DMA(()),
            pltpu.SemaphoreType.DMA(()),
            pltpu.SemaphoreType.DMA((4,)),
        ],
    )(*far(ids, x, gate, up))


def half_kernel(x_ref, out_ref):
    out_ref[...] = x_ref[...]


def half_of(x, place):
    return pl.pallas_call(
        half_kernel,
        name="half",
        compiler_params=LIMIT,
        grid=(1,),
        out_shape=pltpu.VMEM((1024, 256), BF16),
        in_specs=[pl.BlockSpec((1024, 256), lambda i: (place, 0))],
        out_specs=pl.BlockSpec((1024, 256), lambda i: (0, 0)),
    )(x)


def front_kernel(inner_ref, value_ref, x_ref, gate_ref, up_ref, product_ref, tail_ref, hidden_ref):
    product = (inner_ref[...].astype(F32) * value_ref[...].astype(F32)).astype(BF16)
    product_ref[...] = product
    tail_ref[...] = product[126:128]
    gate = jnp.dot(x_ref[...], gate_ref[...], preferred_element_type=F32)
    up = jnp.dot(x_ref[...], up_ref[...], preferred_element_type=F32)
    hidden_ref[...] = (gate / (1.0 + jnp.exp(-gate)) * up).astype(BF16)


def front(*arrays):
    return pl.pallas_call(
        front_kernel,
        name="front",
        compiler_params=LIMIT,
        out_shape=[
            pltpu.VMEM((128, 128), BF16),
            pltpu.VMEM((2, 128), BF16),
            pltpu.VMEM((128, 128), BF16),
        ],
        in_specs=vmem(5),
        out_specs=vmem(3),
    )(*arrays)


def copies_kernel(a_ref, border_ref, product_ref, outer_ref, taps_ref, shared_ref, out_ref, rows_ref):
    rows_ref[6:8, :] = border_ref[...].astype(F32)
    rows_ref[8:136, :] = product_ref[...].astype(F32)
    convolved = jnp.zeros((128, 128), F32)
    for tap in range(3):
        convolved = convolved + taps_ref[tap : tap + 1, :].astype(F32) * rows_ref[6 + tap : 134 + tap, :]
    weighted = (outer_ref[...].astype(F32) * convolved).astype(BF16)
    for q in range(4):
        out_ref[q, 0:768, :] = a_ref[...]
        out_ref[q, 768:896, :] = weighted
        out_ref[q, 896:1024, :] = shared_ref[...]


def copies(arrived, border, product, outer, taps, shared):
    return pl.pallas_call(
        copies_kernel,
        name="copies",
        compiler_params=LIMIT,
        out_shape=pltpu.HBM((4, 1024, 128), BF16),
        in_specs=vmem(6),
        out_specs=vmem(1)[0],
        scratch_shapes=[pltpu.VMEM((136, 128), F32)],
    )(*near(arrived, border, product), outer, taps, *near(shared))


def hidden_kernel(x_ref, own_ref, w1_ref, w2_ref, low_ref, high_ref, out_ref, rest_ref, wide_ref, rows_ref):
    for q in range(4):
        wide_ref[...] = x_ref[q, 0:768, :].astype(F32)
        for b in range(4):
            rows_ref[:, (q * 4 + b) * 128 : (q * 4 + b + 1) * 128] = wide_ref[
                pl.ds(b, 192, stride=4), :
            ].astype(BF16)
        rest_ref[q] = x_ref[q, 768:1024, :]
    for r in range(4):
        if r < 3:
            ref = (own_ref, w1_ref, w2_ref)[r]
            both = jnp.dot(rows_ref[...], ref[...], preferred_element_type=F32)
        else:
            both = jnp.dot(
                rows_ref[:, 0:1024], low_ref[...], preferred_element_type=F32
            ) + jnp.dot(rows_ref[:, 1024:2048], high_ref[...], preferred_element_type=F32)
        gate, up = both[:, 0:128], both[:, 128:256]
        hidden = (gate / (1.0 + jnp.exp(-gate)) * up).astype(BF16)
        for q in range(4):
            out_ref[q, :, r * 128 : (r + 1) * 128] = hidden


def hidden_of(x, *weights):
    return pl.pallas_call(
        hidden_kernel,
        name="hidden",
        compiler_params=LIMIT,
        out_shape=[pltpu.HBM((4, 192, 512), BF16), pltpu.VMEM((4, 256, 128), BF16)],
        in_specs=vmem(6),
        out_specs=vmem(2),
        scratch_shapes=[pltpu.VMEM((768, 128), F32), pltpu.VMEM((192, 2048), BF16)],
    )(*near(x), *weights)


def held_by(r):
    return (lax.axis_index("y") + (0, 3, 1, 2)[r]) % 4


def down_kernel(h_ref, w0_ref, w1_ref, w2_ref, w3_ref, out_ref, rows_ref):
    for r in range(4):
        for q in range(4):
            rows_ref[:, chunk(held_by(r) * 4 + q, 128)] = h_ref[q, :, r * 128 : (r + 1) * 128]
    to, of = iota((256, 192), 0), iota((256, 192), 1)
    place = ((to // 8 == of // SLOTS) & (to % 8 == of % SLOTS)).astype(BF16)
    for b, w_ref in enumerate((w0_ref, w1_ref, w2_ref, w3_ref)):
        total = jnp.dot(rows_ref[...], w_ref[0], preferred_element_type=F32)
        placed = jnp.dot(place, total.astype(BF16), preferred_element_type=F32)
        out_ref[:, held_by(b)] = placed.astype(BF16).reshape(32, 8, 128)


def down_of(h, *weights):
    return pl.pallas_call(
        down_kernel,
        name="down",
        compiler_params=LIMIT,
        out_shape=pltpu.HBM((32, 4, 8, 128), BF16),
        in_specs=vmem(5),
        out_specs=vmem(1)[0],
        scratch_shapes=[pltpu.VMEM((192, 2048), BF16)],
    )(*near(h), *weights)


def wide_kernel(own_ref, n1_ref, n2_ref, n3_ref, mix_ref, shared_ref, mixed_ref, sum_ref):
    for half, (w_ref, out_ref) in enumerate(((mix_ref, mixed_ref), (shared_ref, sum_ref))):
        total = jnp.zeros((128, 128), F32)
        for r, ref in enumerate((own_ref, n1_ref, n2_ref, n3_ref)):
            start = half * 128
            for q in range(4):
                total = total + jnp.dot(
                    ref[q, start : start + 128, :],
                    w_ref[chunk(held_by(r) * 4 + q, 128), :],
                    preferred_element_type=F32,
                )
        out_ref[...] = total


def wide_products(own, n1, n2, n3, mix_out, shared_down):
    return pl.pallas_call(
        wide_kernel,
        name="wide",
        compiler_params=LIMIT,
        out_shape=[pltpu.VMEM((128, 128), F32)] * 2,
        in_specs=vmem(6),
        out_specs=vmem(2),
    )(*near(own, n1, n2, n3), mix_out, shared_down)


def gates_kernel(ids_ref, weights_ref, out_ref):
    ids = ids_ref[...]
    code, experts = ordinals(ids)
    weight = jnp.zeros(experts.shape, F32)
    for k in range(ids.shape[0]):
        weight = weight + jnp.where(ids[k : k + 1, :] == experts, weights_ref[k : k + 1, :], 0.0)
    expert_of, spread = spread_over(code, 1024, 32)
    row = iota(spread.shape, 0)
    wanted = row % 32 // 8 * SLOTS + row % 8 + 1
    here = (spread == wanted.astype(F32)) & (row % 8 < SLOTS)
    for place in range(3):
        piece = weight.astype(BF16)
        weight = weight - piece.astype(F32)
        piece = jnp.dot(expert_of, piece, preferred_element_type=F32)
        out_ref[place] = jnp.where(here, piece, 0.0).astype(BF16)


def gates_of(ids, weights):
    return pl.pallas_call(
        gates_kernel,
        name="gates",
        compiler_params=LIMIT,
        out_shape=pltpu.VMEM((3, 1024, 128), BF16),
        in_specs=vmem(2),
        out_specs=vmem(1)[0],
    )(ids, weights)


def combine_kernel(gates_ref, back_ref, shared_ref, mixed_ref, combined_ref, out_ref):
    back = back_ref[...].reshape(1024, 128)
    routed = jnp.zeros((128, 128), F32)
    for place in (2, 1, 0):
        routed = routed + lax.dot_general(
            gates_ref[place], back, (((0,), (0,)), ((), ())), preferred_element_type=F32
        )
    combined = routed + shared_ref[...]
    combined_ref[...] = combined
    for place, values in ((0, mixed_ref[...]), (2, combined)):
        turned = values.T
        total = jnp.sum(turned, axis=0, keepdims=True)
        square = jnp.sum(turned * turned, axis=0, keepdims=True)
        for p in range(16):
            out_ref[p, place : place + 1, :] = total
            out_ref[p, place + 1 : place + 2, :] = square


def combine(gates, back, shared, mixed):
    return pl.pallas_call(
        combine_kernel,
        name="combine",
        compiler_params=LIMIT,
        out_shape=[pltpu.VMEM((128, 128), F32), pltpu.HBM((16, 4, 128), F32)],
        in_specs=vmem(4),
        out_specs=vmem(2),
    )(*near(gates, back, shared, mixed))


def finish_kernel(stats_ref, mixed_ref, combined_ref, coef_ref, out_mixer_ref, out_experts_ref):
    totals = stats_ref[0]
    for p in range(1, 16):
        totals = totals + stats_ref[p]
    totals = totals / 2048.0
    for place, values_ref, out_ref in (
        (0, mixed_ref, out_mixer_ref),
        (2, combined_ref, out_experts_ref),
    ):
        average = totals[place : place + 1]
        spread = totals[place + 1 : place + 2] - average * average
        scale = lax.rsqrt(spread + 1e-05)
        average = jnp.broadcast_to(average, (128, 128)).T
        scale = jnp.broadcast_to(scale, (128, 128)).T
        scaled = (values_ref[...] - average) * scale
        out_ref[...] = (
            scaled * coef_ref[place : place + 1, :] + coef_ref[place + 1 : place + 2, :]
        ).astype(BF16)


def finish(stats, mixed, combined, coef):
    return pl.pallas_call(
        finish_kernel,
        name="finish",
        compiler_params=LIMIT,
        out_shape=[jax.ShapeDtypeStruct((128, 128), BF16)] * 2,
        in_specs=vmem(4),
        out_specs=vmem(2),
    )(*near(stats, mixed, combined), coef)


def on_device(
    outer_gate,
    inner_gate,
    conv_value,
    conv_taps,
    mix_out,
    gain_mixer,
    bias_mixer,
    moe_input,
    route_ids,
    route_weights,
    expert_gate,
    expert_up,
    expert_down,
    shared_gate,
    shared_up,
    shared_down,
    gain_experts,
    bias_experts,
):
    ep_count = lax.axis_size("ep")
    ids = route_ids.T
    gate_own, up_own = expert_gate.reshape(2048, 128), expert_up.reshape(2048, 128)
    sent, own = pack(ids, moe_input, gate_own, up_own)
    arrived = exchanged(sent.reshape(ep_count, 24, 128), "ep").reshape(768, 128)
    before, after = rotated(own, 1), rotated(own, -1)
    far_low = half_of(before, 0)
    far_high = half_of(after, 1)
    low, high = rotated(far_low, 1), rotated(far_high, -1)
    down1, down2 = rotated(expert_down, 1), rotated(expert_down, -1)
    down3 = rotated(expert_down, 2)

    product, tail, shared_hidden = front(
        inner_gate, conv_value, moe_input, shared_gate, shared_up
    )
    border = shifted(tail, "ep", 1)
    rows = copies(arrived, border, product, outer_gate, conv_taps, shared_hidden)
    rows = exchanged(rows, "x")
    hidden, wide = hidden_of(rows, own, before, after, low, high)
    hidden = exchanged(hidden, "x")
    mixed, shared_sum = wide_products(
        wide, rotated(wide, 1), rotated(wide, -1), rotated(wide, 2), mix_out, shared_down
    )
    expert_out = down_of(hidden, expert_down, down1, down2, down3)
    back = exchanged(expert_out.reshape(ep_count * 4, 8, 128), ("ep", "y"))
    combined, stats = combine(gates_of(ids, route_weights.T), back, shared_sum, mixed)
    stats = exchanged(stats, TP)
    coef = jnp.stack([gain_mixer, bias_mixer, gain_experts, bias_experts]).astype(F32)
    return tuple(finish(stats, mixed, combined, coef))


def solution(mesh):
    split = Mesh(mesh.devices.reshape(mesh.shape["ep"], 4, 4), ("ep", "y", "x"))
    placed = (
        P("ep", TP),
        P("ep", TP),
        P("ep", TP),
        P(None, TP),
        P(None, TP),
        P(TP),
        P(TP),
        P("ep", None),
        P("ep", None),
        P("ep", None),
        P("ep", None, TP),
        P("ep", None, TP),
        P("ep", None, TP),
        P(None, TP),
        P(None, TP),
        P(None, TP),
        P(TP),
        P(TP),
    )
    return jax.shard_map(
        on_device,
        mesh=split,
        in_specs=placed,
        out_specs=(P("ep", TP), P("ep", TP)),
        check_vma=False,
    )
```

```python
import jax
import jax.numpy as jnp
from jax import lax
from jax.experimental import pallas as pl
from jax.experimental.pallas import tpu as pltpu
from jax.sharding import Mesh
from jax.sharding import PartitionSpec as P


F32 = jnp.float32
BF16 = jnp.bfloat16
TP = ("y", "x")
LIMIT = pltpu.CompilerParams(vmem_limit_bytes=20 * 2**20)


def shifted(block, axis, distance):
    devices = range(lax.axis_size(axis))
    route = [(i - distance, i) for i in devices if i - distance in devices]
    return lax.ppermute(block, axis, route)


def rotated(x, distance):
    count = lax.axis_size("y")
    return lax.ppermute(x, "y", [(i, (i + distance) % count) for i in range(count)])


def exchanged(x, axis):
    return lax.all_to_all(x, axis, split_axis=0, concat_axis=0, tiled=True)


def vmem(count):
    return [pl.BlockSpec(memory_space=pltpu.VMEM) for _ in range(count)]


def near(*arrays):
    return [pltpu.with_memory_space_constraint(a, pltpu.VMEM) for a in arrays]


def iota(shape, dim):
    return lax.broadcasted_iota(jnp.int32, shape, dim)


def chunk(index, size):
    return pl.ds(pl.multiple_of(index * size, size), size)


SLOTS, BLOCKS = 6, 4


def ordinals(ids):
    tokens = ids.shape[1]
    experts = iota((32, tokens), 0)
    named = jnp.zeros((32, tokens), F32)
    for k in range(ids.shape[0]):
        named = named + (ids[k : k + 1, :] == experts).astype(F32)
    before = (iota((tokens, tokens), 0) <= iota((tokens, tokens), 1)).astype(BF16)
    place = jnp.dot(named.astype(BF16), before, preferred_element_type=F32)
    return (named * place).astype(BF16), experts


def spread_over(code, rows, each):
    expert_of = (iota((rows, 32), 0) // each == iota((rows, 32), 1)).astype(BF16)
    return expert_of, jnp.dot(expert_of, code, preferred_element_type=F32)


def side_by_side(gate_hbm, up_hbm, stack_ref, sems):
    return tuple(
        pltpu.make_async_copy(
            ref.at[half * 1024 : half * 1024 + 1024],
            stack_ref.at[half * 1024 : half * 1024 + 1024, side * 128 : side * 128 + 128],
            sems.at[2 * side + half],
        )
        for side, ref in enumerate((gate_hbm, up_hbm))
        for half in range(2)
    )


def far(*arrays):
    return [pltpu.with_memory_space_constraint(a, pltpu.HBM) for a in arrays]


def hbm(count):
    return [pl.BlockSpec(memory_space=pltpu.HBM) for _ in range(count)]


def pack_kernel(
    ids_hbm, x_hbm, gate_hbm, up_hbm, out_ref, stack_ref, ids_ref, x_ref, first_sem, sem, sems
):
    first = pltpu.make_async_copy(ids_hbm, ids_ref, first_sem)
    first.start()
    mine = pltpu.make_async_copy(x_hbm.at[:, chunk(lax.axis_index("x"), 512)], x_ref, sem)
    mine.start()
    moves = side_by_side(gate_hbm, up_hbm, stack_ref, sems)
    for move in moves:
        move.start()
    first.wait()
    code, _ = ordinals(ids_ref[...])
    _, spread = spread_over(code, 32 * SLOTS * BLOCKS, SLOTS * BLOCKS)
    wanted = iota(spread.shape, 0) % (SLOTS * BLOCKS) // BLOCKS + (lax.axis_index("y") * SLOTS + 1)
    here = (spread == wanted.astype(F32)).astype(BF16)
    mine.wait()
    taken = jnp.dot(here, x_ref[...], preferred_element_type=F32)
    part = iota(out_ref.shape, 0) % BLOCKS
    out = taken[:, 0:128]
    for b in range(1, BLOCKS):
        out = jnp.where(part == b, taken[:, b * 128 : (b + 1) * 128], out)
    out_ref[...] = out.astype(BF16)
    for move in moves:
        move.wait()


def pack(ids, x, gate, up):
    return pl.pallas_call(
        pack_kernel,
        name="pack",
        compiler_params=LIMIT,
        out_shape=[pltpu.HBM((768, 128), BF16), pltpu.VMEM((2048, 256), BF16)],
        in_specs=hbm(4),
        out_specs=vmem(2),
        scratch_shapes=[
            pltpu.VMEM((4, 128), jnp.int32),
            pltpu.VMEM((128, 512), BF16),
            pltpu.SemaphoreType.DMA(()),
            pltpu.SemaphoreType.DMA(()),
            pltpu.SemaphoreType.DMA((4,)),
        ],
    )(*far(ids, x, gate, up))


def front_kernel(inner_ref, value_ref, x_ref, gate_ref, up_ref, product_ref, tail_ref, hidden_ref):
    product = (inner_ref[...].astype(F32) * value_ref[...].astype(F32)).astype(BF16)
    product_ref[...] = product
    tail_ref[...] = product[126:128]
    gate = jnp.dot(x_ref[...], gate_ref[...], preferred_element_type=F32)
    up = jnp.dot(x_ref[...], up_ref[...], preferred_element_type=F32)
    hidden_ref[...] = (gate / (1.0 + jnp.exp(-gate)) * up).astype(BF16)


def front(*arrays):
    return pl.pallas_call(
        front_kernel,
        name="front",
        compiler_params=LIMIT,
        out_shape=[
            pltpu.VMEM((128, 128), BF16),
            pltpu.VMEM((2, 128), BF16),
            pltpu.VMEM((128, 128), BF16),
        ],
        in_specs=vmem(5),
        out_specs=vmem(3),
    )(*arrays)


def copies_kernel(a_ref, border_ref, product_ref, outer_ref, taps_ref, shared_ref, out_ref, rows_ref):
    rows_ref[6:8, :] = border_ref[...].astype(F32)
    rows_ref[8:136, :] = product_ref[...].astype(F32)
    convolved = jnp.zeros((128, 128), F32)
    for tap in range(3):
        convolved = convolved + taps_ref[tap : tap + 1, :].astype(F32) * rows_ref[6 + tap : 134 + tap, :]
    weighted = (outer_ref[...].astype(F32) * convolved).astype(BF16)
    for q in range(4):
        out_ref[q, 0:768, :] = a_ref[...]
        out_ref[q, 768:896, :] = weighted
        out_ref[q, 896:1024, :] = shared_ref[...]


def copies(arrived, border, product, outer, taps, shared):
    return pl.pallas_call(
        copies_kernel,
        name="copies",
        compiler_params=LIMIT,
        out_shape=pltpu.HBM((4, 1024, 128), BF16),
        in_specs=vmem(6),
        out_specs=vmem(1)[0],
        scratch_shapes=[pltpu.VMEM((136, 128), F32)],
    )(*near(arrived, border, product), outer, taps, *near(shared))


def hidden_kernel(x_ref, own_ref, w1_ref, w2_ref, w3_ref, out_ref, rest_ref, wide_ref, rows_ref):
    for q in range(4):
        wide_ref[...] = x_ref[q, 0:768, :].astype(F32)
        for b in range(4):
            rows_ref[:, (q * 4 + b) * 128 : (q * 4 + b + 1) * 128] = wide_ref[
                pl.ds(b, 192, stride=4), :
            ].astype(BF16)
        rest_ref[q] = x_ref[q, 768:1024, :]
    for r, ref in enumerate((own_ref, w1_ref, w2_ref, w3_ref)):
        both = jnp.dot(rows_ref[...], ref[...], preferred_element_type=F32)
        gate, up = both[:, 0:128], both[:, 128:256]
        hidden = (gate / (1.0 + jnp.exp(-gate)) * up).astype(BF16)
        for q in range(4):
            out_ref[q, :, r * 128 : (r + 1) * 128] = hidden


def hidden_of(x, *weights):
    return pl.pallas_call(
        hidden_kernel,
        name="hidden",
        compiler_params=LIMIT,
        out_shape=[pltpu.HBM((4, 192, 512), BF16), pltpu.VMEM((4, 256, 128), BF16)],
        in_specs=vmem(5),
        out_specs=vmem(2),
        scratch_shapes=[pltpu.VMEM((768, 128), F32), pltpu.VMEM((192, 2048), BF16)],
    )(*near(x), *weights)


def held_by(r):
    return (lax.axis_index("y") + (0, 3, 1, 2)[r]) % 4


def down_kernel(h_ref, w0_ref, w1_ref, w2_ref, w3_ref, out_ref, rows_ref):
    for r in range(4):
        for q in range(4):
            rows_ref[:, chunk(held_by(r) * 4 + q, 128)] = h_ref[q, :, r * 128 : (r + 1) * 128]
    to, of = iota((256, 192), 0), iota((256, 192), 1)
    place = ((to // 8 == of // SLOTS) & (to % 8 == of % SLOTS)).astype(BF16)
    for b, w_ref in enumerate((w0_ref, w1_ref, w2_ref, w3_ref)):
        total = jnp.dot(rows_ref[...], w_ref[0], preferred_element_type=F32)
        placed = jnp.dot(place, total.astype(BF16), preferred_element_type=F32)
        out_ref[:, held_by(b)] = placed.astype(BF16).reshape(32, 8, 128)


def down_of(h, *weights):
    return pl.pallas_call(
        down_kernel,
        name="down",
        compiler_params=LIMIT,
        out_shape=pltpu.HBM((32, 4, 8, 128), BF16),
        in_specs=vmem(5),
        out_specs=vmem(1)[0],
        scratch_shapes=[pltpu.VMEM((192, 2048), BF16)],
    )(*near(h), *weights)


def wide_kernel(own_ref, n1_ref, n2_ref, n3_ref, mix_ref, shared_ref, mixed_ref, sum_ref):
    for half, (w_ref, out_ref) in enumerate(((mix_ref, mixed_ref), (shared_ref, sum_ref))):
        total = jnp.zeros((128, 128), F32)
        for r, ref in enumerate((own_ref, n1_ref, n2_ref, n3_ref)):
            start = half * 128
            for q in range(4):
                total = total + jnp.dot(
                    ref[q, start : start + 128, :],
                    w_ref[chunk(held_by(r) * 4 + q, 128), :],
                    preferred_element_type=F32,
                )
        out_ref[...] = total


def wide_products(own, n1, n2, n3, mix_out, shared_down):
    return pl.pallas_call(
        wide_kernel,
        name="wide",
        compiler_params=LIMIT,
        out_shape=[pltpu.VMEM((128, 128), F32)] * 2,
        in_specs=vmem(6),
        out_specs=vmem(2),
    )(*near(own, n1, n2, n3), mix_out, shared_down)


def gates_kernel(ids_ref, weights_ref, out_ref):
    ids = ids_ref[...]
    code, experts = ordinals(ids)
    weight = jnp.zeros(experts.shape, F32)
    for k in range(ids.shape[0]):
        weight = weight + jnp.where(ids[k : k + 1, :] == experts, weights_ref[k : k + 1, :], 0.0)
    expert_of, spread = spread_over(code, 1024, 32)
    row = iota(spread.shape, 0)
    wanted = row % 32 // 8 * SLOTS + row % 8 + 1
    here = (spread == wanted.astype(F32)) & (row % 8 < SLOTS)
    for place in range(3):
        piece = weight.astype(BF16)
        weight = weight - piece.astype(F32)
        piece = jnp.dot(expert_of, piece, preferred_element_type=F32)
        out_ref[place] = jnp.where(here, piece, 0.0).astype(BF16)


def gates_of(ids, weights):
    return pl.pallas_call(
        gates_kernel,
        name="gates",
        compiler_params=LIMIT,
        out_shape=pltpu.VMEM((3, 1024, 128), BF16),
        in_specs=vmem(2),
        out_specs=vmem(1)[0],
    )(ids, weights)


def combine_kernel(gates_ref, back_ref, shared_ref, mixed_ref, combined_ref, out_ref):
    back = back_ref[...].reshape(1024, 128)
    routed = jnp.zeros((128, 128), F32)
    for place in (2, 1, 0):
        routed = routed + lax.dot_general(
            gates_ref[place], back, (((0,), (0,)), ((), ())), preferred_element_type=F32
        )
    combined = routed + shared_ref[...]
    combined_ref[...] = combined
    for place, values in ((0, mixed_ref[...]), (2, combined)):
        turned = values.T
        total = jnp.sum(turned, axis=0, keepdims=True)
        square = jnp.sum(turned * turned, axis=0, keepdims=True)
        for p in range(16):
            out_ref[p, place : place + 1, :] = total
            out_ref[p, place + 1 : place + 2, :] = square


def combine(gates, back, shared, mixed):
    return pl.pallas_call(
        combine_kernel,
        name="combine",
        compiler_params=LIMIT,
        out_shape=[pltpu.VMEM((128, 128), F32), pltpu.HBM((16, 4, 128), F32)],
        in_specs=vmem(4),
        out_specs=vmem(2),
    )(*near(gates, back, shared, mixed))


def finish_kernel(stats_ref, mixed_ref, combined_ref, coef_ref, out_mixer_ref, out_experts_ref):
    totals = stats_ref[0]
    for p in range(1, 16):
        totals = totals + stats_ref[p]
    totals = totals / 2048.0
    for place, values_ref, out_ref in (
        (0, mixed_ref, out_mixer_ref),
        (2, combined_ref, out_experts_ref),
    ):
        average = totals[place : place + 1]
        spread = totals[place + 1 : place + 2] - average * average
        scale = lax.rsqrt(spread + 1e-05)
        average = jnp.broadcast_to(average, (128, 128)).T
        scale = jnp.broadcast_to(scale, (128, 128)).T
        scaled = (values_ref[...] - average) * scale
        out_ref[...] = (
            scaled * coef_ref[place : place + 1, :] + coef_ref[place + 1 : place + 2, :]
        ).astype(BF16)


def finish(stats, mixed, combined, coef):
    return pl.pallas_call(
        finish_kernel,
        name="finish",
        compiler_params=LIMIT,
        out_shape=[jax.ShapeDtypeStruct((128, 128), BF16)] * 2,
        in_specs=vmem(4),
        out_specs=vmem(2),
    )(*near(stats, mixed, combined), coef)


def on_device(
    outer_gate,
    inner_gate,
    conv_value,
    conv_taps,
    mix_out,
    gain_mixer,
    bias_mixer,
    moe_input,
    route_ids,
    route_weights,
    expert_gate,
    expert_up,
    expert_down,
    shared_gate,
    shared_up,
    shared_down,
    gain_experts,
    bias_experts,
):
    ep_count = lax.axis_size("ep")
    ids = route_ids.T
    gate_own, up_own = expert_gate.reshape(2048, 128), expert_up.reshape(2048, 128)
    sent, own = pack(ids, moe_input, gate_own, up_own)
    arrived = exchanged(sent.reshape(ep_count, 24, 128), "ep").reshape(768, 128)
    before, after = rotated(own, 1), rotated(own, -1)
    beyond = rotated(before, 1)
    down1, down2 = rotated(expert_down, 1), rotated(expert_down, -1)
    down3 = rotated(down2, -1)

    product, tail, shared_hidden = front(
        inner_gate, conv_value, moe_input, shared_gate, shared_up
    )
    border = shifted(tail, "ep", 1)
    rows = copies(arrived, border, product, outer_gate, conv_taps, shared_hidden)
    rows = exchanged(rows, "x")
    hidden, wide = hidden_of(rows, own, before, after, beyond)
    hidden = exchanged(hidden, "x")
    mixed, shared_sum = wide_products(
        wide, rotated(wide, 1), rotated(wide, -1), rotated(wide, 2), mix_out, shared_down
    )
    expert_out = down_of(hidden, expert_down, down1, down2, down3)
    back = exchanged(expert_out.reshape(ep_count * 4, 8, 128), ("ep", "y"))
    combined, stats = combine(gates_of(ids, route_weights.T), back, shared_sum, mixed)
    stats = exchanged(stats, TP)
    coef = jnp.stack([gain_mixer, bias_mixer, gain_experts, bias_experts]).astype(F32)
    return tuple(finish(stats, mixed, combined, coef))


def solution(mesh):
    split = Mesh(mesh.devices.reshape(mesh.shape["ep"], 4, 4), ("ep", "y", "x"))
    placed = (
        P("ep", TP),
        P("ep", TP),
        P("ep", TP),
        P(None, TP),
        P(None, TP),
        P(TP),
        P(TP),
        P("ep", None),
        P("ep", None),
        P("ep", None),
        P("ep", None, TP),
        P("ep", None, TP),
        P("ep", None, TP),
        P(None, TP),
        P(None, TP),
        P(None, TP),
        P(TP),
        P(TP),
    )
    return jax.shard_map(
        on_device,
        mesh=split,
        in_specs=placed,
        out_specs=(P("ep", TP), P("ep", TP)),
        check_vma=False,
    )
```

```python
import jax
import jax.numpy as jnp
from jax import lax
from jax.experimental import pallas as pl
from jax.experimental.pallas import tpu as pltpu
from jax.sharding import Mesh
from jax.sharding import PartitionSpec as P


F32 = jnp.float32
BF16 = jnp.bfloat16
TP = ("y", "x")
LIMIT = pltpu.CompilerParams(vmem_limit_bytes=20 * 2**20)


def shifted(block, axis, distance):
    devices = range(lax.axis_size(axis))
    route = [(i - distance, i) for i in devices if i - distance in devices]
    return lax.ppermute(block, axis, route)


def rotated(x, distance):
    count = lax.axis_size("y")
    return lax.ppermute(x, "y", [(i, (i + distance) % count) for i in range(count)])


def exchanged(x, axis):
    return lax.all_to_all(x, axis, split_axis=0, concat_axis=0, tiled=True)


def vmem(count):
    return [pl.BlockSpec(memory_space=pltpu.VMEM) for _ in range(count)]


def near(*arrays):
    return [pltpu.with_memory_space_constraint(a, pltpu.VMEM) for a in arrays]


def iota(shape, dim):
    return lax.broadcasted_iota(jnp.int32, shape, dim)


def chunk(index, size):
    return pl.ds(pl.multiple_of(index * size, size), size)


SLOTS, BLOCKS = 6, 4


def ordinals(ids):
    tokens = ids.shape[1]
    experts = iota((32, tokens), 0)
    named = jnp.zeros((32, tokens), F32)
    for k in range(ids.shape[0]):
        named = named + (ids[k : k + 1, :] == experts).astype(F32)
    before = (iota((tokens, tokens), 0) <= iota((tokens, tokens), 1)).astype(BF16)
    place = jnp.dot(named.astype(BF16), before, preferred_element_type=F32)
    return (named * place).astype(BF16), experts


def spread_over(code, rows, each):
    expert_of = (iota((rows, 32), 0) // each == iota((rows, 32), 1)).astype(BF16)
    return expert_of, jnp.dot(expert_of, code, preferred_element_type=F32)


def side_by_side(gate_hbm, up_hbm, stack_ref, sems):
    return tuple(
        pltpu.make_async_copy(
            ref.at[half * 1024 : half * 1024 + 1024],
            stack_ref.at[half * 1024 : half * 1024 + 1024, side * 128 : side * 128 + 128],
            sems.at[2 * side + half],
        )
        for side, ref in enumerate((gate_hbm, up_hbm))
        for half in range(2)
    )


def far(*arrays):
    return [pltpu.with_memory_space_constraint(a, pltpu.HBM) for a in arrays]


def hbm(count):
    return [pl.BlockSpec(memory_space=pltpu.HBM) for _ in range(count)]


def pack_kernel(
    ids_hbm, x_hbm, gate_hbm, up_hbm, out_ref, stack_ref, ids_ref, x_ref, first_sem, sem, sems
):
    first = pltpu.make_async_copy(ids_hbm, ids_ref, first_sem)
    first.start()
    mine = pltpu.make_async_copy(x_hbm.at[:, chunk(lax.axis_index("x"), 512)], x_ref, sem)
    mine.start()
    moves = side_by_side(gate_hbm, up_hbm, stack_ref, sems)
    for move in moves:
        move.start()
    first.wait()
    code, _ = ordinals(ids_ref[...])
    _, spread = spread_over(code, 32 * SLOTS * BLOCKS, SLOTS * BLOCKS)
    wanted = iota(spread.shape, 0) % (SLOTS * BLOCKS) // BLOCKS + (lax.axis_index("y") * SLOTS + 1)
    here = (spread == wanted.astype(F32)).astype(BF16)
    mine.wait()
    taken = jnp.dot(here, x_ref[...], preferred_element_type=F32)
    part = iota(out_ref.shape, 0) % BLOCKS
    out = taken[:, 0:128]
    for b in range(1, BLOCKS):
        out = jnp.where(part == b, taken[:, b * 128 : (b + 1) * 128], out)
    out_ref[...] = out.astype(BF16)
    for move in moves:
        move.wait()


def pack(ids, x, gate, up):
    return pl.pallas_call(
        pack_kernel,
        name="pack",
        compiler_params=LIMIT,
        out_shape=[pltpu.HBM((768, 128), BF16), pltpu.VMEM((2048, 256), BF16)],
        in_specs=hbm(4),
        out_specs=vmem(2),
        scratch_shapes=[
            pltpu.VMEM((4, 128), jnp.int32),
            pltpu.VMEM((128, 512), BF16),
            pltpu.SemaphoreType.DMA(()),
            pltpu.SemaphoreType.DMA(()),
            pltpu.SemaphoreType.DMA((4,)),
        ],
    )(*far(ids, x, gate, up))


def front_kernel(
    inner_ref, value_ref, x_ref, gate_ref, up_ref, taps_ref, product_ref, tail_ref, hidden_ref, wide_ref
):
    wide_ref[...] = taps_ref[...].astype(F32)
    product = (inner_ref[...].astype(F32) * value_ref[...].astype(F32)).astype(BF16)
    product_ref[...] = product
    tail_ref[...] = product[126:128]
    gate = jnp.dot(x_ref[...], gate_ref[...], preferred_element_type=F32)
    up = jnp.dot(x_ref[...], up_ref[...], preferred_element_type=F32)
    hidden_ref[...] = (gate / (1.0 + jnp.exp(-gate)) * up).astype(BF16)


def front(*arrays):
    return pl.pallas_call(
        front_kernel,
        name="front",
        compiler_params=LIMIT,
        out_shape=[
            pltpu.VMEM((128, 128), BF16),
            pltpu.VMEM((2, 128), BF16),
            pltpu.VMEM((128, 128), BF16),
            pltpu.VMEM((3, 128), F32),
        ],
        in_specs=vmem(6),
        out_specs=vmem(4),
    )(*arrays)


def copies_kernel(a_ref, border_ref, product_ref, outer_ref, taps_ref, shared_ref, out_ref, rows_ref):
    rows_ref[6:8, :] = border_ref[...].astype(F32)
    rows_ref[8:136, :] = product_ref[...].astype(F32)
    convolved = jnp.zeros((128, 128), F32)
    for tap in range(3):
        convolved = convolved + taps_ref[tap : tap + 1, :] * rows_ref[6 + tap : 134 + tap, :]
    weighted = (outer_ref[...].astype(F32) * convolved).astype(BF16)
    for q in range(4):
        out_ref[q, 0:768, :] = a_ref[...]
        out_ref[q, 768:896, :] = weighted
        out_ref[q, 896:1024, :] = shared_ref[...]


def copies(arrived, border, product, outer, taps, shared):
    return pl.pallas_call(
        copies_kernel,
        name="copies",
        compiler_params=LIMIT,
        out_shape=pltpu.HBM((4, 1024, 128), BF16),
        in_specs=vmem(6),
        out_specs=vmem(1)[0],
        scratch_shapes=[pltpu.VMEM((136, 128), F32)],
    )(*near(arrived, border, product), outer, *near(taps, shared))


def hidden_kernel(x_ref, own_ref, w1_ref, w2_ref, w3_ref, out_ref, rest_ref, wide_ref, rows_ref):
    for q in range(4):
        wide_ref[...] = x_ref[q, 0:768, :].astype(F32)
        for b in range(4):
            rows_ref[:, (q * 4 + b) * 128 : (q * 4 + b + 1) * 128] = wide_ref[
                pl.ds(b, 192, stride=4), :
            ].astype(BF16)
        rest_ref[q] = x_ref[q, 768:1024, :]
    for r, ref in enumerate((own_ref, w1_ref, w2_ref, w3_ref)):
        both = jnp.dot(rows_ref[...], ref[...], preferred_element_type=F32)
        gate, up = both[:, 0:128], both[:, 128:256]
        hidden = (gate / (1.0 + jnp.exp(-gate)) * up).astype(BF16)
        for q in range(4):
            out_ref[q, :, r * 128 : (r + 1) * 128] = hidden


def hidden_of(x, *weights):
    return pl.pallas_call(
        hidden_kernel,
        name="hidden",
        compiler_params=LIMIT,
        out_shape=[pltpu.HBM((4, 192, 512), BF16), pltpu.VMEM((4, 256, 128), BF16)],
        in_specs=vmem(5),
        out_specs=vmem(2),
        scratch_shapes=[pltpu.VMEM((768, 128), F32), pltpu.VMEM((192, 2048), BF16)],
    )(*near(x), *weights)


def held_by(r):
    return (lax.axis_index("y") + (0, 3, 1, 2)[r]) % 4


def down_kernel(h_ref, w0_ref, w1_ref, w2_ref, w3_ref, out_ref, rows_ref):
    for r in range(4):
        for q in range(4):
            rows_ref[:, chunk(held_by(r) * 4 + q, 128)] = h_ref[q, :, r * 128 : (r + 1) * 128]
    to, of = iota((256, 192), 0), iota((256, 192), 1)
    place = ((to // 8 == of // SLOTS) & (to % 8 == of % SLOTS)).astype(BF16)
    for b, w_ref in enumerate((w0_ref, w1_ref, w2_ref, w3_ref)):
        total = jnp.dot(rows_ref[...], w_ref[0], preferred_element_type=F32)
        placed = jnp.dot(place, total.astype(BF16), preferred_element_type=F32)
        out_ref[:, held_by(b)] = placed.astype(BF16).reshape(32, 8, 128)


def down_of(h, *weights):
    return pl.pallas_call(
        down_kernel,
        name="down",
        compiler_params=LIMIT,
        out_shape=pltpu.HBM((32, 4, 8, 128), BF16),
        in_specs=vmem(5),
        out_specs=vmem(1)[0],
        scratch_shapes=[pltpu.VMEM((192, 2048), BF16)],
    )(*near(h), *weights)


def wide_kernel(own_ref, n1_ref, n2_ref, n3_ref, mix_ref, shared_ref, mixed_ref, sum_ref):
    for half, (w_ref, out_ref) in enumerate(((mix_ref, mixed_ref), (shared_ref, sum_ref))):
        total = jnp.zeros((128, 128), F32)
        for r, ref in enumerate((own_ref, n1_ref, n2_ref, n3_ref)):
            start = half * 128
            for q in range(4):
                total = total + jnp.dot(
                    ref[q, start : start + 128, :],
                    w_ref[chunk(held_by(r) * 4 + q, 128), :],
                    preferred_element_type=F32,
                )
        out_ref[...] = total


def wide_products(own, n1, n2, n3, mix_out, shared_down):
    return pl.pallas_call(
        wide_kernel,
        name="wide",
        compiler_params=LIMIT,
        out_shape=[pltpu.VMEM((128, 128), F32)] * 2,
        in_specs=vmem(6),
        out_specs=vmem(2),
    )(*near(own, n1, n2, n3), mix_out, shared_down)


def gates_kernel(ids_ref, weights_ref, out_ref):
    ids = ids_ref[...]
    code, experts = ordinals(ids)
    weight = jnp.zeros(experts.shape, F32)
    for k in range(ids.shape[0]):
        weight = weight + jnp.where(ids[k : k + 1, :] == experts, weights_ref[k : k + 1, :], 0.0)
    expert_of, spread = spread_over(code, 1024, 32)
    row = iota(spread.shape, 0)
    wanted = row % 32 // 8 * SLOTS + row % 8 + 1
    here = (spread == wanted.astype(F32)) & (row % 8 < SLOTS)
    for place in range(3):
        piece = weight.astype(BF16)
        weight = weight - piece.astype(F32)
        piece = jnp.dot(expert_of, piece, preferred_element_type=F32)
        out_ref[place] = jnp.where(here, piece, 0.0).astype(BF16)


def gates_of(ids, weights):
    return pl.pallas_call(
        gates_kernel,
        name="gates",
        compiler_params=LIMIT,
        out_shape=pltpu.VMEM((3, 1024, 128), BF16),
        in_specs=vmem(2),
        out_specs=vmem(1)[0],
    )(ids, weights)


def combine_kernel(gates_ref, back_ref, shared_ref, mixed_ref, combined_ref, out_ref):
    back = back_ref[...].reshape(1024, 128)
    routed = jnp.zeros((128, 128), F32)
    for place in (2, 1, 0):
        routed = routed + lax.dot_general(
            gates_ref[place], back, (((0,), (0,)), ((), ())), preferred_element_type=F32
        )
    combined = routed + shared_ref[...]
    combined_ref[...] = combined
    for place, values in ((0, mixed_ref[...]), (2, combined)):
        turned = values.T
        total = jnp.sum(turned, axis=0, keepdims=True)
        square = jnp.sum(turned * turned, axis=0, keepdims=True)
        for p in range(16):
            out_ref[p, place : place + 1, :] = total
            out_ref[p, place + 1 : place + 2, :] = square


def combine(gates, back, shared, mixed):
    return pl.pallas_call(
        combine_kernel,
        name="combine",
        compiler_params=LIMIT,
        out_shape=[pltpu.VMEM((128, 128), F32), pltpu.HBM((16, 4, 128), F32)],
        in_specs=vmem(4),
        out_specs=vmem(2),
    )(*near(gates, back, shared, mixed))


def finish_kernel(stats_ref, mixed_ref, combined_ref, coef_ref, out_mixer_ref, out_experts_ref):
    totals = stats_ref[0]
    for p in range(1, 16):
        totals = totals + stats_ref[p]
    totals = totals / 2048.0
    for place, values_ref, out_ref in (
        (0, mixed_ref, out_mixer_ref),
        (2, combined_ref, out_experts_ref),
    ):
        average = totals[place : place + 1]
        spread = totals[place + 1 : place + 2] - average * average
        scale = lax.rsqrt(spread + 1e-05)
        average = jnp.broadcast_to(average, (128, 128)).T
        scale = jnp.broadcast_to(scale, (128, 128)).T
        scaled = (values_ref[...] - average) * scale
        out_ref[...] = (
            scaled * coef_ref[place : place + 1, :] + coef_ref[place + 1 : place + 2, :]
        ).astype(BF16)


def finish(stats, mixed, combined, coef):
    return pl.pallas_call(
        finish_kernel,
        name="finish",
        compiler_params=LIMIT,
        out_shape=[jax.ShapeDtypeStruct((128, 128), BF16)] * 2,
        in_specs=vmem(4),
        out_specs=vmem(2),
    )(*near(stats, mixed, combined), coef)


def on_device(
    outer_gate,
    inner_gate,
    conv_value,
    conv_taps,
    mix_out,
    gain_mixer,
    bias_mixer,
    moe_input,
    route_ids,
    route_weights,
    expert_gate,
    expert_up,
    expert_down,
    shared_gate,
    shared_up,
    shared_down,
    gain_experts,
    bias_experts,
):
    ep_count = lax.axis_size("ep")
    ids = route_ids.T
    gate_own, up_own = expert_gate.reshape(2048, 128), expert_up.reshape(2048, 128)
    sent, own = pack(ids, moe_input, gate_own, up_own)
    arrived = exchanged(sent.reshape(ep_count, 24, 128), "ep").reshape(768, 128)
    before, after = rotated(own, 1), rotated(own, -1)
    beyond = rotated(before, 1)
    down1, down2 = rotated(expert_down, 1), rotated(expert_down, -1)
    down3 = rotated(down2, -1)

    product, tail, shared_hidden, taps = front(
        inner_gate, conv_value, moe_input, shared_gate, shared_up, conv_taps
    )
    border = shifted(tail, "ep", 1)
    rows = copies(arrived, border, product, outer_gate, taps, shared_hidden)
    rows = exchanged(rows, "x")
    hidden, wide = hidden_of(rows, own, before, after, beyond)
    hidden = exchanged(hidden, "x")
    mixed, shared_sum = wide_products(
        wide, rotated(wide, 1), rotated(wide, -1), rotated(wide, 2), mix_out, shared_down
    )
    expert_out = down_of(hidden, expert_down, down1, down2, down3)
    back = exchanged(expert_out.reshape(ep_count * 4, 8, 128), ("ep", "y"))
    combined, stats = combine(gates_of(ids, route_weights.T), back, shared_sum, mixed)
    stats = exchanged(stats, TP)
    coef = jnp.stack([gain_mixer, bias_mixer, gain_experts, bias_experts]).astype(F32)
    return tuple(finish(stats, mixed, combined, coef))


def solution(mesh):
    split = Mesh(mesh.devices.reshape(mesh.shape["ep"], 4, 4), ("ep", "y", "x"))
    placed = (
        P("ep", TP),
        P("ep", TP),
        P("ep", TP),
        P(None, TP),
        P(None, TP),
        P(TP),
        P(TP),
        P("ep", None),
        P("ep", None),
        P("ep", None),
        P("ep", None, TP),
        P("ep", None, TP),
        P("ep", None, TP),
        P(None, TP),
        P(None, TP),
        P(None, TP),
        P(TP),
        P(TP),
    )
    return jax.shard_map(
        on_device,
        mesh=split,
        in_specs=placed,
        out_specs=(P("ep", TP), P("ep", TP)),
        check_vma=False,
    )
```
